32 devices in a mesh: tp: 16 (over z, y, x), dp: 2 (over core).
Axes of the slice: x: 2, y: 2, z: 4, core: 2. Of those that a mesh axis runs over, the one named last changes fastest.
Arguments:
- tokens: bfloat16 [64, 4096], P(None, 'dp'), may hold values from -6 to 6
- lengths: int32 [64], P('dp'), may hold values from 1 to 4096, 65536 in all
- norm_gain: float32 [2, 4096], P(None, 'dp'), may hold values from 0.1 to 1.9
- w_in: bfloat16 [2, 4096, 2048], P(None, 'dp', 'tp'), may hold values from -0.09375 to 0.09375
- log_step: float32 [2, 128], P(None, 'tp'), may hold values from -4.6 to -0.7
- eig_re: float32 [2, 128, 64], P(None, 'tp'), may hold values from -2 to -0.05
- eig_im: float32 [2, 128, 64], P(None, 'tp'), may hold values from 0 to 8
- in_mat: float32 [2, 2, 128, 64, 16], P(None, None, 'tp'), may hold values from -2.5 to 2.5
- output_matrices: float32 [2, 2, 128, 16, 64], P(None, None, 'tp'), may hold values from -1.25 to 1.25
- skip: float32 [2, 2048], P(None, 'tp'), may hold values from -4 to 4
- w_glu: bfloat16 [2, 2048, 4096], P(None, 'tp', 'dp'), may hold values from -0.375 to 0.375
- w_gate: bfloat16 [2, 2048, 4096], P(None, 'tp', 'dp'), may hold values from -0.125 to 0.125
- state: float32 [2, 2, 64, 8192], P(None, None, 'dp', 'tp'), may hold values from -6 to 6
Outputs:
- mixed: bfloat16 [64, 4096], P(None, 'dp')
- new_state: float32 [2, 2, 64, 8192], P(None, None, 'dp', 'tp')
The draws below stay inside these ranges and needn't reach their ends.
Inputs may be any that keep to these rules, and one draw needn't show every extreme that they name: `lengths`: each sequence's number of past positions; the largest is exactly 4096 and all add up to 65536.
All inputs are finite; a program needn't handle non-finite values.
Results may differ from the reference program's by a relative error of at most 0.0095.
Values may be sent and summed in bfloat16 or wider, within the bound.
No kernel may reach another device: no remote copies, remote signals or barrier semaphores. Data moves between devices by JAX's collectives and lax.ppermute only.
A program may use at most 64 MiB of HBM per device.

```python
import math
import jax
import jax.numpy as jnp
import numpy as np
from jax import lax

D = 4096
GROUPS = 128
GROUP = 16
STATES = 64
S5W = 2048
LAYERS = 2
BATCH = 64
LEN_MAX = 4096
LEN_MEAN = 1024
BLOCK_LEN = 256


def spiked(array, stream_key, source, target, shards_of, factor):
    owner, partner = [(jnp.arange(array.shape[dim]) // (array.shape[dim] // shards_of)).reshape([-1 if axis == dim else 1 for axis in range(array.ndim)]) for dim in (source, target)]
    chosen = jax.random.permutation(stream_key, shards_of)[partner]
    strong = (owner == chosen) | (owner == (partner + shards_of // 2) % shards_of)
    return jnp.where(strong, factor * array, array)


def block_levels(own_key, dims, pieces, low, top_value):
    def one(position, shards_of):
        draws = jax.random.uniform(jax.random.fold_in(jax.random.fold_in(own_key, 6), position), (shards_of,), jnp.float32, low / len(pieces), top_value / len(pieces))
        return jnp.repeat(jnp.exp(draws), dims[position] // shards_of).reshape((-1,) + (1,) * (len(dims) - position - 1))

    level = one(*pieces[0])
    for cut in pieces[1:]:
        level = level * one(*cut)
    return level


def profile(number_of, total, reach, lean):
    loads = [(1 << 20) // math.isqrt(grade ** lean) + 1 for grade in range(2, number_of + 1)]
    rest, holding = total - reach - (number_of - 1), [1] * (number_of - 1)
    while rest > 0:
        candidates = [i for i in range(number_of - 1) if holding[i] < reach]
        mass, remaining = sum([loads[i] for i in candidates]), rest
        for i in candidates:
            extra = min(reach - holding[i], max(1, remaining * loads[i] // mass), rest)
            holding[i] = holding[i] + extra
            rest = rest - extra
    return np.array([reach] + holding)


def ragged(rng, amount, total, reach, skew):
    if amount == 2:
        one = jax.random.randint(rng, (), max(1, total - reach), min(reach, total - 1) + 1)
        return jnp.stack([one, total - one])
    sizes = jnp.asarray(profile(amount, total, reach, skew), jnp.int32)
    couples = (amount - 1) // 2
    giver, sink = sizes[1:1 + 2 * couples:2], sizes[2:2 + 2 * couples:2]
    slack = jnp.minimum(giver - 1, reach - sink)
    moved = jax.random.randint(jax.random.fold_in(rng, 1), (couples,), 0, 1 << 20) % (slack + 1)
    sizes = sizes.at[1:1 + 2 * couples:2].set(giver - moved).at[2:2 + 2 * couples:2].set(sink + moved)
    return sizes[jax.random.permutation(jax.random.fold_in(rng, 2), amount)]


def scatter_about(rng, extent, spread, limit, split=(), kind=jnp.bfloat16):
    result = spread * jax.random.normal(rng, extent, jnp.float32)
    if split:
        result = result * block_levels(rng, extent, split, -0.22, 0.18)
    return jnp.clip(result, -limit, limit).astype(kind)


def noise_with(key, dims, deviation, most, pieces, heavy, kind=jnp.bfloat16):
    entries = deviation * jax.random.normal(key, dims, jnp.float32)
    if pieces:
        entries = entries * block_levels(key, dims, pieces, -0.22, 0.18)
    return jnp.clip(spiked(entries, jax.random.fold_in(key, 3), *heavy), -most, most).astype(kind)


def setup_inputs(seed: int = 0) -> dict:
    arg_keys = jax.random.split(jax.random.key(seed), 14)
    return {
        "tokens": scatter_about(arg_keys[0], (BATCH, D), 1.0, 6.0, ((1, 2),)),
        "lengths": ragged(arg_keys[1], BATCH, BATCH * LEN_MEAN, LEN_MAX, 2).astype(jnp.int32),
        "norm_gain": jnp.clip(1.0 + 0.18 * jax.random.normal(arg_keys[2], (LAYERS, D), jnp.float32), 0.1, 1.9),
        "w_in": scatter_about(arg_keys[3], (LAYERS, D, S5W), D ** -0.5, 0.09375, ((1, 2), (2, 16))),
        "log_step": jnp.clip(-4.6 + 3.8999999 * jax.random.uniform(arg_keys[4], (LAYERS, GROUPS), jnp.float32) ** block_levels(arg_keys[4], (LAYERS, GROUPS), ((1, 16),), -0.2, 0.2), -4.6, -0.7),
        "eig_re": jnp.clip(-2.0 + 1.95 * jax.random.uniform(arg_keys[5], (LAYERS, GROUPS, STATES), jnp.float32) ** block_levels(arg_keys[5], (LAYERS, GROUPS, STATES), ((1, 16),), -0.2, 0.2), -2.0, -0.05),
        "eig_im": jnp.clip(8.0 * jax.random.uniform(arg_keys[6], (LAYERS, GROUPS, STATES), jnp.float32) ** block_levels(arg_keys[6], (LAYERS, GROUPS, STATES), ((1, 16),), -0.2, 0.2), 0.0, 8.0),
        "in_mat": scatter_about(arg_keys[7], (LAYERS, 2, GROUPS, STATES, GROUP), 0.177, 2.5, ((2, 16),), jnp.float32),
        "output_matrices": scatter_about(arg_keys[8], (LAYERS, 2, GROUPS, GROUP, STATES), 0.088, 1.25, ((2, 16),), jnp.float32),
        "skip": scatter_about(arg_keys[9], (LAYERS, S5W), 1.0, 4.0, ((1, 16),), jnp.float32),
        "w_glu": noise_with(arg_keys[10], (LAYERS, S5W, D), (S5W // 4) ** -0.5, 0.375, ((1, 16), (2, 2)), (1, 2, 16, 2.0)),
        "w_gate": scatter_about(arg_keys[11], (LAYERS, S5W, D), S5W ** -0.5, 0.125, ((1, 16), (2, 2))),
        "state": scatter_about(arg_keys[12], (LAYERS, 2, BATCH, GROUPS * STATES), 0.5, 6.0, ((2, 2), (3, 16)), jnp.float32),
    }


NORM_EPS = 1e-06
FULL_PRECISION = lax.Precision.HIGHEST

def position_factor(lengths):
    blocks = (lengths // BLOCK_LEN).astype(jnp.float32)
    return 2.0 / (1.0 + blocks * (4.0 * BLOCK_LEN / LEN_MAX))

def recurrent_step(driven_state, state_pair, factor, log_step, eig_re, eig_im, in_mat, output_matrices, skip):
    step_size = jnp.exp(log_step)[None, :, None] * factor[:, None, None]
    magnitude = jnp.exp(eig_re[None] * step_size)
    turned = eig_im[None] * step_size
    decay_re = magnitude * jnp.cos(turned)
    decay_im = magnitude * jnp.sin(turned)
    modulus = eig_re * eig_re + eig_im * eig_im
    weight_re = ((decay_re - 1.0) * eig_re + decay_im * eig_im) / modulus
    weight_im = (decay_im * eig_re - (decay_re - 1.0) * eig_im) / modulus
    drive_re = jnp.einsum('bgc,gpc->bgp', driven_state, in_mat[0], precision=FULL_PRECISION)
    drive_im = jnp.einsum('bgc,gpc->bgp', driven_state, in_mat[1], precision=FULL_PRECISION)
    state_real = decay_re * state_pair[0] - decay_im * state_pair[1] + weight_re * drive_re - weight_im * drive_im
    state_imaginary = decay_re * state_pair[1] + decay_im * state_pair[0] + weight_re * drive_im + weight_im * drive_re
    readout_value = jnp.einsum('szv,zuv->szu', state_real, output_matrices[0], precision=FULL_PRECISION) - jnp.einsum('szv,zuv->szu', state_imaginary, output_matrices[1], precision=FULL_PRECISION) + skip * driven_state
    return (jax.nn.gelu(readout_value), state_real, state_imaginary)

def reference(tokens, lengths, norm_gain, w_in, log_step, eig_re, eig_im, in_mat, output_matrices, skip, w_glu, w_gate, state):
    factor = position_factor(lengths)
    current = tokens.astype(jnp.float32)
    rounded = tokens
    new_states = []
    for layer_index in range(LAYERS):
        squares = lax.optimization_barrier(jnp.sum(current * current, axis=1))
        scaled = (current * norm_gain[layer_index]).astype(jnp.bfloat16)
        partial_value = jnp.dot(scaled, w_in[layer_index], preferred_element_type=jnp.float32)
        driven_state = (partial_value * lax.rsqrt(squares / D + NORM_EPS)[:, None]).astype(jnp.bfloat16)
        driven_state = driven_state.astype(jnp.float32).reshape(BATCH, GROUPS, GROUP)
        state_pair = state[layer_index].reshape(2, BATCH, GROUPS, STATES)
        readout_value, state_real, state_imaginary = recurrent_step(driven_state, state_pair, factor, log_step[layer_index], eig_re[layer_index], eig_im[layer_index], in_mat[layer_index], output_matrices[layer_index], skip[layer_index].reshape(GROUPS, GROUP))
        readout_value = readout_value.reshape(BATCH, GROUPS * GROUP).astype(jnp.bfloat16)
        new_states.append(jnp.stack([state_real, state_imaginary]).reshape(2, BATCH, GROUPS * STATES))
        linear = jnp.dot(readout_value, w_glu[layer_index], preferred_element_type=jnp.float32)
        gate_sum = jnp.dot(readout_value, w_gate[layer_index], preferred_element_type=jnp.float32)
        rounded = (current + linear * jax.nn.sigmoid(gate_sum)).astype(jnp.bfloat16)
        current = rounded.astype(jnp.float32)
    return (rounded, jnp.stack(new_states))
```

```python
import math

import jax
import jax.numpy as jnp
from jax import lax
from jax.sharding import PartitionSpec as P

BLOCK_LEN = 256
LEN_MAX = 4096
NORM_EPS = 1e-06
FULL_PRECISION = lax.Precision.HIGHEST


def position_factor(lengths):
    blocks = (lengths // BLOCK_LEN).astype(jnp.float32)
    return 2.0 / (1.0 + blocks * (4.0 * BLOCK_LEN / LEN_MAX))


def shifted(value, axis, size, stride, count, hop):
    pairs = []
    for i in range(size):
        digit = (i // stride) % count
        pairs.append((i, i + ((digit + hop) % count - digit) * stride))
    return lax.ppermute(value, axis, pairs)


def coefficients(factor, log_step, eig_re, eig_im):
    step_size = jnp.exp(log_step)[None, :, None] * factor[:, None, None]
    magnitude = jnp.exp(eig_re[None] * step_size)
    turned = eig_im[None] * step_size
    decay_re = magnitude * jnp.cos(turned)
    decay_im = magnitude * jnp.sin(turned)
    modulus = eig_re * eig_re + eig_im * eig_im
    weight_re = ((decay_re - 1.0) * eig_re + decay_im * eig_im) / modulus
    weight_im = (decay_im * eig_re - (decay_re - 1.0) * eig_im) / modulus
    return decay_re, decay_im, weight_re, weight_im


def recurrent_step(driven_state, state_pair, coeffs, in_mat, output_matrices, skip):
    decay_re, decay_im, weight_re, weight_im = coeffs
    drive_re = jnp.einsum("bgc,gpc->bgp", driven_state, in_mat[0], precision=FULL_PRECISION)
    drive_im = jnp.einsum("bgc,gpc->bgp", driven_state, in_mat[1], precision=FULL_PRECISION)
    state_real = (
        decay_re * state_pair[0]
        - decay_im * state_pair[1]
        + weight_re * drive_re
        - weight_im * drive_im
    )
    state_imaginary = (
        decay_re * state_pair[1]
        + decay_im * state_pair[0]
        + weight_re * drive_im
        + weight_im * drive_re
    )
    readout_value = (
        jnp.einsum("szv,zuv->szu", state_real, output_matrices[0], precision=FULL_PRECISION)
        - jnp.einsum("szv,zuv->szu", state_imaginary, output_matrices[1], precision=FULL_PRECISION)
        + skip * driven_state
    )
    return (jax.nn.gelu(readout_value), state_real, state_imaginary)


def make_body(tp, dp):
    inner = 1 << (int(math.log2(tp)) // 2)
    outer = tp // inner

    def body(
        tokens,
        lengths,
        norm_gain,
        w_in,
        log_step,
        eig_re,
        eig_im,
        in_mat,
        output_matrices,
        skip,
        w_glu,
        w_gate,
        state,
    ):
        layers = w_in.shape[0]
        seqs, feats = tokens.shape
        own = seqs // dp
        model = feats * dp
        groups = log_step.shape[1]
        width = skip.shape[1]
        group = width // groups
        states = eig_re.shape[2]
        chunk = feats // tp
        me = lax.axis_index("dp")
        place = lax.axis_index("tp")
        low, high = place % inner, place // inner

        factor = position_factor(lengths)

        glu_parts = [w_glu] + [shifted(w_glu, "dp", dp, 1, dp, -k) for k in range(1, dp)]
        gate_parts = [w_gate] + [shifted(w_gate, "dp", dp, 1, dp, -k) for k in range(1, dp)]
        in_parts = [w_in] + [shifted(w_in, "dp", dp, 1, dp, -k) for k in range(1, dp)]
        gain_parts = [norm_gain] + [shifted(norm_gain, "dp", dp, 1, dp, -k) for k in range(1, dp)]

        token_rows = tokens.reshape(dp, own, feats)

        def rows_of(k):
            return lax.dynamic_index_in_dim(token_rows, (me + k) % dp, 0, keepdims=False)

        parts = [rows_of(0)] + [shifted(rows_of(dp - k), "dp", dp, 1, dp, -k) for k in range(1, dp)]
        mine = [
            lax.dynamic_slice_in_dim(p, place * chunk, chunk, axis=1).astype(jnp.float32)
            for p in parts
        ]
        new_states = []
        rounded = None
        for layer in range(layers):
            coeffs = coefficients(factor, log_step[layer], eig_re[layer], eig_im[layer])
            squares = 0.0
            partial_value = 0.0
            for k in range(dp):
                current = parts[k].astype(jnp.float32)
                squares = squares + jnp.sum(current * current, axis=1)
                scaled = (current * gain_parts[k][layer]).astype(jnp.bfloat16)
                partial_value = partial_value + jnp.dot(
                    scaled, in_parts[k][layer], preferred_element_type=jnp.float32
                )
            driven = (partial_value * lax.rsqrt(squares / model + NORM_EPS)[:, None]).astype(
                jnp.bfloat16
            )
            driven = driven.astype(jnp.float32).reshape(own, groups, group)
            state_pair = state[layer].reshape(2, own, groups, states)
            readout, state_real, state_imaginary = recurrent_step(
                driven,
                state_pair,
                coeffs,
                in_mat[layer],
                output_matrices[layer],
                skip[layer].reshape(groups, group),
            )
            readout = readout.reshape(own, width).astype(jnp.bfloat16)
            new_states.append(
                jnp.stack([state_real, state_imaginary]).reshape(2, own, groups * states)
            )
            terms = []
            for weights in (glu_parts, gate_parts):
                for k in range(dp):
                    term = jnp.dot(readout, weights[k][layer], preferred_element_type=jnp.float32)
                    terms.append(term.reshape(own, outer, inner, chunk))
            terms = jnp.concatenate(terms, axis=3)

            def to_low(k):
                return lax.dynamic_index_in_dim(terms, (low + k) % inner, 2, keepdims=False)

            total = to_low(0)
            arrived = [
                shifted(to_low(k).astype(jnp.bfloat16), "tp", tp, 1, inner, k)
                for k in range(1, inner)
            ]
            for value in arrived:
                total = total + value.astype(jnp.float32)

            def to_high(k):
                return lax.dynamic_index_in_dim(total, (high + k) % outer, 1, keepdims=False)

            block = to_high(0)
            arrived = [
                shifted(to_high(k).astype(jnp.bfloat16), "tp", tp, inner, outer, k)
                for k in range(1, outer)
            ]
            for value in arrived:
                block = block + value.astype(jnp.float32)
            linear, gate = block[:, : dp * chunk], block[:, dp * chunk :]
            before = jnp.concatenate(mine, axis=1)
            after = (before + linear * jax.nn.sigmoid(gate)).astype(jnp.bfloat16)

            if layer + 1 < layers:
                shard = after
            else:
                pieces = [after[:, k * chunk : (k + 1) * chunk] for k in range(dp)]
                here = [pieces[0]] + [
                    shifted(pieces[k], "dp", dp, 1, dp, k) for k in range(1, dp)
                ]
                here = jnp.stack(here)
                order = (me - jnp.arange(dp)) % dp
                shard = here[order].reshape(seqs, chunk)

            rows = shard.shape[0]
            column = [shard] + [
                shifted(shard, "tp", tp, inner, outer, -k) for k in range(1, outer)
            ]
            column = jnp.stack(column)
            turn = (jnp.arange(outer) - high) % outer
            whole_column = jnp.stack(
                [lax.dynamic_index_in_dim(column, turn[h], 0, keepdims=False) for h in range(outer)]
            )
            plane = [whole_column] + [
                shifted(whole_column, "tp", tp, 1, inner, -k) for k in range(1, inner)
            ]
            plane = jnp.stack(plane)
            gathered = jnp.stack(
                [
                    lax.dynamic_index_in_dim(plane, (l - low) % inner, 0, keepdims=False)
                    for l in range(inner)
                ],
                axis=1,
            )
            if layer + 1 < layers:
                gathered = gathered.reshape(tp, rows, dp, chunk).transpose(2, 1, 0, 3)
                parts = [gathered[k].reshape(own, feats) for k in range(dp)]
                mine = [
                    after[:, k * chunk : (k + 1) * chunk].astype(jnp.float32) for k in range(dp)
                ]
            else:
                rounded = gathered.reshape(tp, rows, chunk).transpose(1, 0, 2).reshape(rows, feats)
        return (rounded, jnp.stack(new_states))

    return body


def solution(mesh):
    placed = (
        P(None, "dp"),
        P("dp"),
        P(None, "dp"),
        P(None, "dp", "tp"),
        P(None, "tp"),
        P(None, "tp", None),
        P(None, "tp", None),
        P(None, None, "tp", None, None),
        P(None, None, "tp", None, None),
        P(None, "tp"),
        P(None, "tp", "dp"),
        P(None, "tp", "dp"),
        P(None, None, "dp", "tp"),
    )
    return jax.shard_map(
        make_body(mesh.shape["tp"], mesh.shape["dp"]),
        mesh=mesh,
        in_specs=placed,
        out_specs=(P(None, "dp"), P(None, None, "dp", "tp")),
        check_vma=False,
    )
```

```python
import functools
import math

import jax
import jax.numpy as jnp
from jax import lax
from jax.experimental import pallas as pl
from jax.experimental.pallas import tpu as pltpu
from jax.sharding import PartitionSpec as P

BLOCK_LEN = 256
LEN_MAX = 4096
NORM_EPS = 1e-06
F32 = jnp.float32
BF16 = jnp.bfloat16


def position_factor(lengths):
    blocks = (lengths // BLOCK_LEN).astype(F32)
    return 2.0 / (1.0 + blocks * (4.0 * BLOCK_LEN / LEN_MAX))


def exchange(value, axis, size, stride, count, k):
    pairs = []
    for i in range(size):
        digit = (i // stride) % count
        pairs.append((i, i + ((digit ^ k) - digit) * stride))
    return lax.ppermute(value, axis, pairs)


def params(mib=16):
    return pltpu.CompilerParams(vmem_limit_bytes=mib << 20)


def whole(shape):
    return pl.BlockSpec(shape, lambda i: (0,) * len(shape))


def layer_block(shape, layer):
    return pl.BlockSpec((1,) + shape[1:], lambda i: (layer,) + (0,) * (len(shape) - 1))


SMEM = pl.BlockSpec(memory_space=pltpu.SMEM)


def struct(shape, dtype):
    return jax.ShapeDtypeStruct(shape, dtype)


def nt_dot(a, b):
    return lax.dot_general(a, b, (((1,), (1,)), ((), ())), preferred_element_type=F32)


def prepare_kernel(group, states, factor_ref, rows_ref, in_ref, out_ref, coeff_ref, m_ref, n_ref):
    layers = rows_ref.shape[0]
    total = rows_ref.shape[2]
    width = m_ref.shape[3]
    factor = factor_ref[...]
    spread_in = (
        lax.broadcasted_iota(jnp.int32, (group, width), 1) % group
        == lax.broadcasted_iota(jnp.int32, (group, width), 0)
    ).astype(BF16)
    keep_in = (
        lax.broadcasted_iota(jnp.int32, (total, width), 0) // states
        == lax.broadcasted_iota(jnp.int32, (total, width), 1) // group
    )
    spread_out = (
        lax.broadcasted_iota(jnp.int32, (states, total), 1) % states
        == lax.broadcasted_iota(jnp.int32, (states, total), 0)
    ).astype(BF16)
    keep_out = (
        lax.broadcasted_iota(jnp.int32, (width, total), 0) // group
        == lax.broadcasted_iota(jnp.int32, (width, total), 1) // states
    )
    for layer in range(layers):
        log_step = rows_ref[layer, 0:1, :]
        eig_re = rows_ref[layer, 1:2, :]
        eig_im = rows_ref[layer, 2:3, :]
        step_size = jnp.exp(log_step) * factor
        magnitude = jnp.exp(eig_re * step_size)
        turned = eig_im * step_size
        decay_re = magnitude * jnp.cos(turned)
        decay_im = magnitude * jnp.sin(turned)
        scale = 1.0 / (eig_re * eig_re + eig_im * eig_im)
        coeff_ref[layer, 0] = decay_re
        coeff_ref[layer, 1] = decay_im
        coeff_ref[layer, 2] = ((decay_re - 1.0) * eig_re + decay_im * eig_im) * scale
        coeff_ref[layer, 3] = (decay_im * eig_re - (decay_re - 1.0) * eig_im) * scale
        for part in range(2):
            m = jnp.dot(in_ref[layer, part].astype(BF16), spread_in, preferred_element_type=F32)
            m_ref[layer, part] = jnp.where(keep_in, m, 0.0).astype(BF16)
            n = jnp.dot(out_ref[layer, part].astype(BF16), spread_out, preferred_element_type=F32)
            if part == 1:
                n = -n
            n_ref[layer, part] = jnp.where(keep_out, n, 0.0).astype(BF16)


def prepare(factor, log_step, eig_re, eig_im, in_mat, output_matrices):
    layers, groups, states = eig_re.shape
    group = in_mat.shape[4]
    own = factor.shape[0]
    total, width = groups * states, groups * group
    rows = jnp.stack(
        [
            jnp.broadcast_to(log_step[:, :, None], eig_re.shape).reshape(layers, total),
            eig_re.reshape(layers, total),
            eig_im.reshape(layers, total),
        ],
        axis=1,
    )
    args = (
        factor[:, None],
        rows,
        in_mat.reshape(layers, 2, total, group),
        output_matrices.reshape(layers, 2, width, states),
    )
    outs = [
        struct((layers, 4, own, total), F32),
        struct((layers, 2, total, width), BF16),
        struct((layers, 2, width, total), BF16),
    ]
    return pl.pallas_call(
        functools.partial(prepare_kernel, group, states),
        grid=(1,),
        in_specs=[whole(a.shape) for a in args],
        out_specs=[whole(o.shape) for o in outs],
        out_shape=outs,
        compiler_params=params(),
        cost_estimate=pl.CostEstimate(flops=8 << 20, bytes_accessed=3 << 20, transcendentals=0),
        name="prepare",
    )(*args)


def recur_kernel(layer, dp, inner, outer, model, n_pieces, *refs):
    place_ref = refs[0]
    pieces = refs[1 : 1 + n_pieces]
    gains = refs[1 + n_pieces : 1 + n_pieces + dp]
    weights = refs[1 + n_pieces + dp : 1 + n_pieces + 2 * dp]
    coeff_ref, m_ref, n_ref, skip_ref, state_ref = refs[1 + n_pieces + 2 * dp :][:5]
    readout_ref, new_ref, line = refs[-3:]
    own, feats = line.shape[1:]
    if n_pieces == dp and layer == 0:
        currents = pieces
    else:
        low, high = place_ref[0], place_ref[1]
        chunk = feats // (inner * outer)
        for k in range(inner):
            for h in range(outer):
                at = ((high ^ h) * inner + (low ^ k)) * chunk
                for p in range(dp):
                    line[p, :, pl.ds(pl.multiple_of(at, chunk), chunk)] = pieces[k][
                        h, :, p * chunk : (p + 1) * chunk
                    ]
        currents = [line.at[p] for p in range(dp)]
    squares = jnp.zeros((own, 1), F32)
    partial_value = None
    for p in range(dp):
        current = currents[p][...].astype(F32)
        squares = squares + jnp.sum(current * current, axis=1, keepdims=True)
        scaled = (current * gains[p][layer : layer + 1, :]).astype(BF16)
        term = jnp.dot(scaled, weights[p][0], preferred_element_type=F32)
        partial_value = term if partial_value is None else partial_value + term
    driven = (partial_value * lax.rsqrt(squares / model + NORM_EPS)).astype(BF16)
    drive_re = nt_dot(driven, m_ref[0, 0])
    drive_im = nt_dot(driven, m_ref[0, 1])
    decay_re, decay_im = coeff_ref[0, 0], coeff_ref[0, 1]
    weight_re, weight_im = coeff_ref[0, 2], coeff_ref[0, 3]
    old_re, old_im = state_ref[0, 0], state_ref[0, 1]
    new_re = decay_re * old_re - decay_im * old_im + weight_re * drive_re - weight_im * drive_im
    new_im = decay_re * old_im + decay_im * old_re + weight_re * drive_im + weight_im * drive_re
    new_ref[0, 0] = new_re
    new_ref[0, 1] = new_im
    value = nt_dot(new_re.astype(BF16), n_ref[0, 0]) + nt_dot(new_im.astype(BF16), n_ref[0, 1])
    value = value + skip_ref[layer : layer + 1, :] * driven.astype(F32)
    readout_ref[...] = jax.nn.gelu(value).astype(BF16)


def recur(layer, dims, place, pieces, gains, weights, coeff, m, n, skip, state, so_far):
    dp, inner, outer, model, own, feats = dims
    width = skip.shape[1]
    args = [place, *pieces, *gains, *weights, coeff, m, n, skip, state]
    specs = (
        [SMEM]
        + [whole(p.shape) for p in pieces]
        + [whole(g.shape) for g in gains]
        + [layer_block(w.shape, layer) for w in weights]
        + [layer_block(a.shape, layer) for a in (coeff, m, n)]
        + [whole(skip.shape), layer_block(state.shape, layer)]
    )
    alias = {}
    if so_far is not None:
        alias = {len(args): 1}
        args.append(so_far)
        specs.append(pl.BlockSpec(memory_space=pl.ANY))
    return pl.pallas_call(
        functools.partial(recur_kernel, layer, dp, inner, outer, model, len(pieces)),
        grid=(1,),
        in_specs=specs,
        out_specs=[whole((own, width)), layer_block(state.shape, layer)],
        out_shape=[struct((own, width), BF16), struct(state.shape, F32)],
        scratch_shapes=[pltpu.VMEM((dp, own, feats), BF16)],
        input_output_aliases=alias,
        compiler_params=params(),
        cost_estimate=pl.CostEstimate(flops=64 << 20, bytes_accessed=2 << 20, transcendentals=0),
        name=f"recur_{layer}",
    )(*args)


def product_kernel(inner, outer, chunk, place_ref, readout_ref, *refs):
    count = len(refs) - inner - 1
    weights, outs, spread = refs[:count], refs[count:-1], refs[-1]
    low = place_ref[0]
    readout = readout_ref[...]
    for w in range(count):
        value = jnp.dot(readout, weights[w][0], preferred_element_type=F32)
        for j in range(inner * outer):
            spread[w, j] = value[:, j * chunk : (j + 1) * chunk]
    for k in range(inner):
        for h in range(outer):
            for w in range(count):
                outs[k][h, :, w * chunk : (w + 1) * chunk] = spread[
                    w, h * inner + (low ^ k)
                ].astype(outs[k].dtype)


def products(layer, dims, place, readout, weights):
    dp, inner, outer, model, own, feats = dims
    chunk = feats // (inner * outer)
    count = len(weights)
    shape = (outer, own, count * chunk)
    outs = [struct(shape, F32)] + [struct(shape, BF16)] * (inner - 1)
    return pl.pallas_call(
        functools.partial(product_kernel, inner, outer, chunk),
        grid=(1,),
        in_specs=[SMEM, whole(readout.shape)] + [layer_block(w.shape, layer) for w in weights],
        out_specs=[whole(shape)] * inner,
        out_shape=outs,
        scratch_shapes=[pltpu.VMEM((count, inner * outer, own, chunk), F32)],
        compiler_params=params(),
        cost_estimate=pl.CostEstimate(flops=64 << 20, bytes_accessed=3 << 20, transcendentals=0),
        name=f"products_{layer}",
    )(place, readout, *weights)


def fold_kernel(outer, inner, place_ref, own_ref, *refs):
    arrived, outs = refs[: inner - 1], refs[inner - 1 :]
    high = place_ref[1]
    for k in range(outer):
        at = high ^ k
        total = own_ref[at]
        for ref in arrived:
            total = total + ref[at].astype(F32)
        outs[k][...] = total.astype(outs[k].dtype)


def fold(place, value, arrived):
    outer, own, wide = value.shape
    outs = [struct((own, wide), F32)] + [struct((own, wide), BF16)] * (outer - 1)
    return pl.pallas_call(
        functools.partial(fold_kernel, outer, len(arrived) + 1),
        grid=(1,),
        in_specs=[SMEM] + [whole(value.shape)] * (1 + len(arrived)),
        out_specs=[whole((own, wide))] * outer,
        out_shape=outs,
        compiler_params=params(8),
        cost_estimate=pl.CostEstimate(flops=1 << 20, bytes_accessed=1 << 19, transcendentals=0),
        name="fold",
    )(place, value, *arrived)


def update_kernel(own_ref, before_ref, *refs):
    arrived, out = refs[:-1], refs[-1]
    total = own_ref[...]
    for ref in arrived:
        total = total + ref[...].astype(F32)
    half = total.shape[1] // 2
    linear, gate = total[:, :half], total[:, half:]
    out[...] = (before_ref[...].astype(F32) + linear * jax.nn.sigmoid(gate)).astype(BF16)


def update(block, arrived, before):
    return pl.pallas_call(
        update_kernel,
        grid=(1,),
        in_specs=[whole(block.shape), whole(before.shape)] + [whole(a.shape) for a in arrived],
        out_specs=whole(before.shape),
        out_shape=struct(before.shape, BF16),
        compiler_params=params(8),
        cost_estimate=pl.CostEstimate(flops=1 << 20, bytes_accessed=1 << 18, transcendentals=0),
        name="update",
    )(block, before, *arrived)


def settle_kernel(inner, outer, chunk, place_ref, *refs):
    pieces, out = refs[:-1], refs[-1]
    low, high = place_ref[0], place_ref[1]
    for k in range(inner):
        for h in range(outer):
            at = ((high ^ h) * inner + (low ^ k)) * chunk
            out[:, pl.ds(pl.multiple_of(at, chunk), chunk)] = pieces[k][h]


def settle(place, pieces, feats):
    outer, rows, chunk = pieces[0].shape
    return pl.pallas_call(
        functools.partial(settle_kernel, len(pieces), outer, chunk),
        grid=(1,),
        in_specs=[SMEM] + [whole(p.shape) for p in pieces],
        out_specs=whole((rows, feats)),
        out_shape=struct((rows, feats), BF16),
        compiler_params=params(8),
        name="settle",
    )(place, *pieces)


def plain_prepare(factor, log_step, eig_re, eig_im, in_mat, output_matrices):
    step_size = jnp.exp(log_step)[:, None, :, None] * factor[None, :, None, None]
    eig_re, eig_im = eig_re[:, None], eig_im[:, None]
    magnitude = jnp.exp(eig_re * step_size)
    turned = eig_im * step_size
    decay_re = magnitude * jnp.cos(turned)
    decay_im = magnitude * jnp.sin(turned)
    modulus = eig_re * eig_re + eig_im * eig_im
    weight_re = ((decay_re - 1.0) * eig_re + decay_im * eig_im) / modulus
    weight_im = (decay_im * eig_re - (decay_re - 1.0) * eig_im) / modulus
    return jnp.stack([decay_re, decay_im, weight_re, weight_im], axis=1), in_mat, output_matrices


def plain_order(place, pieces, inner, outer):
    rows = []
    for h in range(outer):
        for l in range(inner):
            row = jnp.stack(pieces)[place[0] ^ l, place[1] ^ h]
            rows.append(row)
    return jnp.stack(rows)


def plain_recur(layer, dims, place, pieces, gains, weights, coeff, m, n, skip, state, so_far):
    dp, inner, outer, model, own, feats = dims
    groups, states = coeff.shape[3:]
    if layer > 0:
        rows = plain_order(place, pieces, inner, outer)
        rows = rows.reshape(inner * outer, own, dp, feats // (inner * outer))
        pieces = [rows[:, :, p].transpose(1, 0, 2).reshape(own, feats) for p in range(dp)]
    squares, partial_value = 0.0, 0.0
    for p in range(dp):
        current = pieces[p].astype(F32)
        squares = squares + jnp.sum(current * current, axis=1, keepdims=True)
        scaled = (current * gains[p][layer]).astype(BF16)
        partial_value = partial_value + jnp.dot(
            scaled, weights[p][layer], preferred_element_type=F32
        )
    driven = (partial_value * lax.rsqrt(squares / model + NORM_EPS)).astype(BF16).astype(F32)
    driven = driven.reshape(own, groups, -1)
    exact = lax.Precision.HIGHEST
    drive_re = jnp.einsum("bgc,gpc->bgp", driven, m[layer, 0], precision=exact)
    drive_im = jnp.einsum("bgc,gpc->bgp", driven, m[layer, 1], precision=exact)
    decay_re, decay_im, weight_re, weight_im = [coeff[layer, c] for c in range(4)]
    old_re, old_im = [state[layer, c].reshape(own, groups, states) for c in range(2)]
    new_re = decay_re * old_re - decay_im * old_im + weight_re * drive_re - weight_im * drive_im
    new_im = decay_re * old_im + decay_im * old_re + weight_re * drive_im + weight_im * drive_re
    value = jnp.einsum("bgp,gcp->bgc", new_re, n[layer, 0], precision=exact)
    value = value - jnp.einsum("bgp,gcp->bgc", new_im, n[layer, 1], precision=exact)
    value = value + skip[layer].reshape(groups, -1) * driven
    readout = jax.nn.gelu(value).reshape(own, -1).astype(BF16)
    new = jnp.stack([new_re, new_im]).reshape(1, 2, own, groups * states)
    if so_far is not None:
        new = jnp.concatenate([so_far, new])
    return readout, new


def plain_products(layer, dims, place, readout, weights):
    dp, inner, outer, model, own, feats = dims
    terms = []
    for w in weights:
        term = jnp.dot(readout, w[layer], preferred_element_type=F32)
        terms.append(term.reshape(own, outer, inner, -1))
    terms = jnp.concatenate(terms, axis=3).transpose(2, 1, 0, 3)
    outs = [terms[place[0] ^ k] for k in range(inner)]
    return [outs[0]] + [o.astype(BF16) for o in outs[1:]]


def plain_fold(place, value, arrived):
    for a in arrived:
        value = value + a.astype(F32)
    outs = [value[place[1] ^ k] for k in range(value.shape[0])]
    return [outs[0]] + [o.astype(BF16) for o in outs[1:]]


def plain_update(block, arrived, before):
    for a in arrived:
        block = block + a.astype(F32)
    half = block.shape[1] // 2
    gated = block[:, :half] * jax.nn.sigmoid(block[:, half:])
    return (before.astype(F32) + gated).astype(BF16)


def plain_settle(place, pieces, feats):
    rows = plain_order(place, pieces, len(pieces), pieces[0].shape[0])
    return rows.transpose(1, 0, 2).reshape(rows.shape[1], feats)


def make_body(tp, dp):
    inner = 1 << (int(math.log2(tp)) // 2)
    outer = tp // inner

    def body(
        tokens,
        lengths,
        norm_gain,
        w_in,
        log_step,
        eig_re,
        eig_im,
        in_mat,
        output_matrices,
        skip,
        w_glu,
        w_gate,
        state,
    ):
        layers = w_in.shape[0]
        seqs, feats = tokens.shape
        own = seqs // dp
        chunk = feats // tp
        dims = (dp, inner, outer, feats * dp, own, feats)
        me = lax.axis_index("dp")
        index = lax.axis_index("tp")
        place = jnp.stack([index % inner, index // inner]).astype(jnp.int32)
        if chunk % 128 == 0 and own % 16 == 0 and skip.shape[1] % 128 == 0:
            stages = (prepare, recur, products, fold, update, settle)
        else:
            stages = (
                plain_prepare,
                plain_recur,
                plain_products,
                plain_fold,
                plain_update,
                plain_settle,
            )
        do_prepare, do_recur, do_products, do_fold, do_update, do_settle = stages

        def slabs(value):
            return [value] + [exchange(value, "dp", dp, 1, dp, k) for k in range(1, dp)]

        def over_low(value, k):
            return exchange(value, "tp", tp, 1, inner, k)

        def over_high(value, k):
            return exchange(value, "tp", tp, inner, outer, k)

        token_rows = tokens.reshape(dp, own, feats)

        def rows_of(k):
            return lax.dynamic_index_in_dim(token_rows, me ^ k, 0, keepdims=False)

        pieces = [rows_of(0)] + [exchange(rows_of(k), "dp", dp, 1, dp, k) for k in range(1, dp)]
        gain_slabs = slabs(norm_gain)
        in_slabs = slabs(w_in)
        glu_slabs = slabs(w_glu)
        gate_slabs = slabs(w_gate)
        before = jnp.concatenate(
            [lax.dynamic_slice_in_dim(p, index * chunk, chunk, axis=1) for p in pieces], axis=1
        )
        coeff, m, n = do_prepare(
            position_factor(lengths), log_step, eig_re, eig_im, in_mat, output_matrices
        )
        new_state = None
        for layer in range(layers):
            readout, new_state = do_recur(
                layer, dims, place, pieces, gain_slabs, in_slabs, coeff, m, n, skip, state, new_state
            )
            sends = do_products(layer, dims, place, readout, glu_slabs + gate_slabs)
            arrived = [over_low(sends[k], k) for k in range(1, inner)]
            sends = do_fold(place, sends[0], arrived)
            arrived = [over_high(sends[k], k) for k in range(1, outer)]
            shard = do_update(sends[0], arrived, before)
            before = shard
            if layer + 1 == layers:
                cuts = [shard[:, k * chunk : (k + 1) * chunk] for k in range(dp)]
                here = jnp.stack(
                    [cuts[0]] + [exchange(cuts[k], "dp", dp, 1, dp, k) for k in range(1, dp)]
                )
                if dp == 2:
                    flip = me == 1
                    shard = jnp.concatenate(
                        [jnp.where(flip, here[1], here[0]), jnp.where(flip, here[0], here[1])]
                    )
                else:
                    shard = here[me ^ jnp.arange(dp)].reshape(seqs, chunk)
            column = jnp.stack([shard] + [over_high(shard, k) for k in range(1, outer)])
            pieces = [column] + [over_low(column, k) for k in range(1, inner)]
        return (do_settle(place, pieces, feats), new_state)

    return body


def solution(mesh):
    placed = (
        P(None, "dp"),
        P("dp"),
        P(None, "dp"),
        P(None, "dp", "tp"),
        P(None, "tp"),
        P(None, "tp", None),
        P(None, "tp", None),
        P(None, None, "tp", None, None),
        P(None, None, "tp", None, None),
        P(None, "tp"),
        P(None, "tp", "dp"),
        P(None, "tp", "dp"),
        P(None, None, "dp", "tp"),
    )
    return jax.shard_map(
        make_body(mesh.shape["tp"], mesh.shape["dp"]),
        mesh=mesh,
        in_specs=placed,
        out_specs=(P(None, "dp"), P(None, None, "dp", "tp")),
        check_vma=False,
    )
```

```python
import functools
import math

import jax
import jax.numpy as jnp
from jax import lax
from jax.experimental import pallas as pl
from jax.experimental.pallas import tpu as pltpu
from jax.sharding import PartitionSpec as P

BLOCK_LEN = 256
LEN_MAX = 4096
NORM_EPS = 1e-06
F32 = jnp.float32
BF16 = jnp.bfloat16


def position_factor(lengths):
    blocks = (lengths // BLOCK_LEN).astype(F32)
    return 2.0 / (1.0 + blocks * (4.0 * BLOCK_LEN / LEN_MAX))


def exchange(value, axis, size, stride, count, k):
    pairs = []
    for i in range(size):
        digit = (i // stride) % count
        pairs.append((i, i + ((digit ^ k) - digit) * stride))
    return lax.ppermute(value, axis, pairs)


def params(mib=16):
    return pltpu.CompilerParams(vmem_limit_bytes=mib << 20)


VMEM = pl.BlockSpec(memory_space=pltpu.VMEM)
ANY = pl.BlockSpec(memory_space=pl.ANY)


def struct(shape, dtype):
    return jax.ShapeDtypeStruct(shape, dtype)


def nt_dot(a, b):
    return lax.dot_general(a, b, (((1,), (1,)), ((), ())), preferred_element_type=F32)


def digits(inner):
    index = lax.axis_index("tp")
    return index % inner, index // inner


def iota(shape, axis):
    return lax.broadcasted_iota(jnp.int32, shape, axis)


def exact_dot(a, b):
    return jnp.dot(a, b, precision=lax.Precision.HIGHEST, preferred_element_type=F32)


def prepare_kernel(
    lengths_ref, step_ref, re_ref, im_ref, in_ref, out_ref, coeff_ref, m_ref, n_ref
):
    layers, groups, states = re_ref.shape
    total, width = coeff_ref.shape[3], n_ref.shape[2]
    group = width // groups
    own = lengths_ref.shape[1]
    row = jnp.broadcast_to(position_factor(lengths_ref[...]), (own, own))
    factor = jnp.sum(
        jnp.where(iota((own, own), 0) == iota((own, own), 1), row, 0.0), axis=1, keepdims=True
    )
    spread = (iota((states, total), 1) % states == iota((states, total), 0)).astype(F32)
    spread_half = spread.astype(BF16)
    of_group = iota((groups, total), 1) // states == iota((groups, total), 0)
    keep = iota((width, total), 0) // group == iota((width, total), 1) // states

    def flat(value):
        return jnp.sum(
            jnp.where(of_group, exact_dot(value, spread), 0.0), axis=0, keepdims=True
        )

    for layer in range(layers):
        log_step = exact_dot(step_ref[layer : layer + 1, :], of_group.astype(F32))
        eig_re = flat(re_ref[layer])
        eig_im = flat(im_ref[layer])
        step_size = jnp.exp(log_step) * factor
        magnitude = jnp.exp(eig_re * step_size)
        turned = eig_im * step_size
        decay_re = magnitude * jnp.cos(turned)
        decay_im = magnitude * jnp.sin(turned)
        scale = 1.0 / (eig_re * eig_re + eig_im * eig_im)
        coeff_ref[layer, 0] = decay_re
        coeff_ref[layer, 1] = decay_im
        coeff_ref[layer, 2] = ((decay_re - 1.0) * eig_re + decay_im * eig_im) * scale
        coeff_ref[layer, 3] = (decay_im * eig_re - (decay_re - 1.0) * eig_im) * scale
        for part in range(2):
            for source, target in ((in_ref, m_ref), (out_ref, n_ref)):
                value = jnp.dot(
                    source[layer, part].astype(BF16), spread_half, preferred_element_type=F32
                )
                if part == 1 and target is n_ref:
                    value = -value
                target[layer, part] = jnp.where(keep, value, 0.0).astype(BF16)


def prepare(lengths, log_step, eig_re, eig_im, in_mat, output_matrices):
    layers, groups, states = eig_re.shape
    group = in_mat.shape[4]
    own = lengths.shape[0]
    total, width = groups * states, groups * group
    args = (
        lengths[None, :],
        log_step,
        eig_re,
        eig_im,
        jnp.swapaxes(in_mat, 3, 4).reshape(layers, 2, width, states),
        output_matrices.reshape(layers, 2, width, states),
    )
    outs = [
        struct((layers, 4, own, total), F32),
        struct((layers, 2, width, total), BF16),
        struct((layers, 2, width, total), BF16),
    ]
    return pl.pallas_call(
        prepare_kernel,
        in_specs=[VMEM] * len(args),
        out_specs=[VMEM] * len(outs),
        out_shape=outs,
        compiler_params=params(8),
        cost_estimate=pl.CostEstimate(flops=8 << 20, bytes_accessed=3 << 20, transcendentals=0),
        name="prepare",
    )(*args)


def recur_kernel(layer, dp, inner, outer, model, n_pieces, *refs):
    pieces = refs[:n_pieces]
    gains = refs[n_pieces : n_pieces + dp]
    weights = refs[n_pieces + dp : n_pieces + 2 * dp]
    coeff_ref, m_ref, n_ref, skip_ref, state_ref = refs[n_pieces + 2 * dp :][:5]
    if layer == 0:
        readout_ref, state_out, before_ref = refs[-6:-3]
    else:
        readout_ref, state_out = refs[-5:-3]
    line, new_ref, sem = refs[-3:]
    own, feats = line.shape[1:]
    chunk = feats // (inner * outer)
    low, high = digits(inner)
    if layer == 0:
        start = pl.multiple_of(lax.axis_index("dp") * own, own)
        at = pl.multiple_of((high * inner + low) * chunk, chunk)
        currents = [p.at[pl.ds(start, own), :] for p in pieces]
        for p in range(dp):
            before_ref[:, p * chunk : (p + 1) * chunk] = pieces[p][
                pl.ds(start, own), pl.ds(at, chunk)
            ]
    else:
        for k in range(inner):
            for h in range(outer):
                at = pl.multiple_of(((high ^ h) * inner + (low ^ k)) * chunk, chunk)
                for p in range(dp):
                    line[p, :, pl.ds(at, chunk)] = pieces[k][h, :, p * chunk : (p + 1) * chunk]
        currents = [line.at[p] for p in range(dp)]
    squares = jnp.zeros((own, 1), F32)
    partial_value = None
    for p in range(dp):
        current = currents[p][...].astype(F32)
        squares = squares + jnp.sum(current * current, axis=1, keepdims=True)
        scaled = (current * gains[p][layer : layer + 1, :]).astype(BF16)
        term = jnp.dot(scaled, weights[p][layer], preferred_element_type=F32)
        partial_value = term if partial_value is None else partial_value + term
    driven = (partial_value * lax.rsqrt(squares / model + NORM_EPS)).astype(BF16)
    drive_re = jnp.dot(driven, m_ref[layer, 0], preferred_element_type=F32)
    drive_im = jnp.dot(driven, m_ref[layer, 1], preferred_element_type=F32)
    decay_re, decay_im = coeff_ref[layer, 0], coeff_ref[layer, 1]
    weight_re, weight_im = coeff_ref[layer, 2], coeff_ref[layer, 3]
    old_re, old_im = state_ref[layer, 0], state_ref[layer, 1]
    new_re = decay_re * old_re - decay_im * old_im + weight_re * drive_re - weight_im * drive_im
    new_im = decay_re * old_im + decay_im * old_re + weight_re * drive_im + weight_im * drive_re
    new_ref[0] = new_re
    new_ref[1] = new_im
    copy = pltpu.make_async_copy(new_ref, state_out.at[layer], sem)
    copy.start()
    value = nt_dot(new_re.astype(BF16), n_ref[layer, 0])
    value = value + nt_dot(new_im.astype(BF16), n_ref[layer, 1])
    value = value + skip_ref[layer : layer + 1, :] * driven.astype(F32)
    readout_ref[...] = jax.nn.gelu(value).astype(BF16)
    copy.wait()


def recur(layer, dims, pieces, gains, weights, coeff, m, n, skip, state, so_far):
    dp, inner, outer, model, own, feats = dims
    width = skip.shape[1]
    args = [*pieces, *gains, *weights, coeff, m, n, skip, state]
    specs = [VMEM] * len(args)
    outs = [struct((own, width), BF16), struct(state.shape, F32)]
    out_specs = [VMEM, ANY]
    alias = {}
    if layer == 0:
        outs.append(struct((own, dp * feats // (inner * outer)), BF16))
        out_specs.append(VMEM)
    else:
        alias = {len(args): 1}
        args.append(so_far)
        specs.append(ANY)
    return pl.pallas_call(
        functools.partial(recur_kernel, layer, dp, inner, outer, model, len(pieces)),
        in_specs=specs,
        out_specs=out_specs,
        out_shape=outs,
        scratch_shapes=[
            pltpu.VMEM((dp, own, feats), BF16),
            pltpu.VMEM(state.shape[1:], F32),
            pltpu.SemaphoreType.DMA,
        ],
        input_output_aliases=alias,
        compiler_params=params(8),
        cost_estimate=pl.CostEstimate(flops=64 << 20, bytes_accessed=2 << 20, transcendentals=0),
        name=f"recur_{layer}",
    )(*args)


def product_kernel(layer, inner, outer, chunk, readout_ref, *refs):
    count = len(refs) - inner - 1
    weights, outs, spread = refs[:count], refs[count:-1], refs[-1]
    low, _ = digits(inner)
    readout = readout_ref[...]
    for w in range(count):
        value = jnp.dot(readout, weights[w][layer], preferred_element_type=F32)
        for j in range(inner * outer):
            spread[w, j] = value[:, j * chunk : (j + 1) * chunk]
    for k in range(inner):
        for h in range(outer):
            for w in range(count):
                outs[k][h, :, w * chunk : (w + 1) * chunk] = spread[
                    w, h * inner + (low ^ k)
                ].astype(outs[k].dtype)


def products(layer, dims, readout, weights):
    dp, inner, outer, model, own, feats = dims
    chunk = feats // (inner * outer)
    count = len(weights)
    shape = (outer, own, count * chunk)
    outs = [struct(shape, F32)] + [struct(shape, BF16)] * (inner - 1)
    return pl.pallas_call(
        functools.partial(product_kernel, layer, inner, outer, chunk),
        in_specs=[VMEM] * (1 + count),
        out_specs=[VMEM] * inner,
        out_shape=outs,
        scratch_shapes=[pltpu.VMEM((count, inner * outer, own, chunk), F32)],
        compiler_params=params(8),
        cost_estimate=pl.CostEstimate(flops=64 << 20, bytes_accessed=3 << 20, transcendentals=0),
        name=f"products_{layer}",
    )(readout, *weights)


def fold_kernel(outer, inner, own_ref, *refs):
    arrived, outs = refs[: inner - 1], refs[inner - 1 :]
    _, high = digits(inner)
    for k in range(outer):
        at = high ^ k
        total = own_ref[at]
        for ref in arrived:
            total = total + ref[at].astype(F32)
        outs[k][...] = total.astype(outs[k].dtype)


def fold(value, arrived):
    outer, own, wide = value.shape
    outs = [struct((own, wide), F32)] + [struct((own, wide), BF16)] * (outer - 1)
    return pl.pallas_call(
        functools.partial(fold_kernel, outer, len(arrived) + 1),
        in_specs=[VMEM] * (1 + len(arrived)),
        out_specs=[VMEM] * outer,
        out_shape=outs,
        compiler_params=params(4),
        cost_estimate=pl.CostEstimate(flops=1 << 20, bytes_accessed=1 << 19, transcendentals=0),
        name="fold",
    )(value, *arrived)


def update_kernel(own_ref, before_ref, *refs):
    arrived, out = refs[:-1], refs[-1]
    total = own_ref[...]
    for ref in arrived:
        total = total + ref[...].astype(F32)
    half = total.shape[1] // 2
    linear, gate = total[:, :half], total[:, half:]
    out[...] = (before_ref[...].astype(F32) + linear * jax.nn.sigmoid(gate)).astype(BF16)


def update(block, arrived, before):
    return pl.pallas_call(
        update_kernel,
        in_specs=[VMEM] * (2 + len(arrived)),
        out_specs=VMEM,
        out_shape=struct(before.shape, BF16),
        compiler_params=params(4),
        cost_estimate=pl.CostEstimate(flops=1 << 20, bytes_accessed=1 << 18, transcendentals=0),
        name="update",
    )(block, before, *arrived)


def settle_kernel(inner, outer, chunk, *refs):
    pieces, out, sem = refs[:-2], refs[-2], refs[-1]
    low, high = digits(inner)
    copies = []
    for k in range(inner):
        for h in range(outer):
            at = pl.multiple_of(((high ^ h) * inner + (low ^ k)) * chunk, chunk)
            copies.append(
                pltpu.make_async_copy(
                    pieces[k].at[h], out.at[:, pl.ds(at, chunk)], sem.at[k * outer + h]
                )
            )
            copies[-1].start()
    for copy in copies:
        copy.wait()


def settle(pieces, feats):
    outer, rows, chunk = pieces[0].shape
    inner = len(pieces)
    return pl.pallas_call(
        functools.partial(settle_kernel, inner, outer, chunk),
        in_specs=[VMEM] * inner,
        out_specs=ANY,
        out_shape=struct((rows, feats), BF16),
        scratch_shapes=[pltpu.SemaphoreType.DMA((inner * outer,))],
        compiler_params=params(4),
        name="settle",
    )(*pieces)


def plain_prepare(lengths, log_step, eig_re, eig_im, in_mat, output_matrices):
    factor = position_factor(lengths)
    step_size = jnp.exp(log_step)[:, None, :, None] * factor[None, :, None, None]
    eig_re, eig_im = eig_re[:, None], eig_im[:, None]
    magnitude = jnp.exp(eig_re * step_size)
    turned = eig_im * step_size
    decay_re = magnitude * jnp.cos(turned)
    decay_im = magnitude * jnp.sin(turned)
    modulus = eig_re * eig_re + eig_im * eig_im
    weight_re = ((decay_re - 1.0) * eig_re + decay_im * eig_im) / modulus
    weight_im = (decay_im * eig_re - (decay_re - 1.0) * eig_im) / modulus
    return jnp.stack([decay_re, decay_im, weight_re, weight_im], axis=1), in_mat, output_matrices


def plain_order(pieces, inner, outer):
    low, high = digits(inner)
    rows = []
    for h in range(outer):
        for l in range(inner):
            row = jnp.stack(pieces)[low ^ l, high ^ h]
            rows.append(row)
    return jnp.stack(rows)


def plain_recur(layer, dims, pieces, gains, weights, coeff, m, n, skip, state, so_far):
    dp, inner, outer, model, own, feats = dims
    groups, states = coeff.shape[3:]
    if layer > 0:
        rows = plain_order(pieces, inner, outer)
        rows = rows.reshape(inner * outer, own, dp, feats // (inner * outer))
        pieces = [rows[:, :, p].transpose(1, 0, 2).reshape(own, feats) for p in range(dp)]
    else:
        start = lax.axis_index("dp") * own
        pieces = [lax.dynamic_slice_in_dim(p, start, own, axis=0) for p in pieces]
    squares, partial_value = 0.0, 0.0
    for p in range(dp):
        current = pieces[p].astype(F32)
        squares = squares + jnp.sum(current * current, axis=1, keepdims=True)
        scaled = (current * gains[p][layer]).astype(BF16)
        partial_value = partial_value + jnp.dot(
            scaled, weights[p][layer], preferred_element_type=F32
        )
    driven = (partial_value * lax.rsqrt(squares / model + NORM_EPS)).astype(BF16).astype(F32)
    driven = driven.reshape(own, groups, -1)
    exact = lax.Precision.HIGHEST
    drive_re = jnp.einsum("bgc,gpc->bgp", driven, m[layer, 0], precision=exact)
    drive_im = jnp.einsum("bgc,gpc->bgp", driven, m[layer, 1], precision=exact)
    decay_re, decay_im, weight_re, weight_im = [coeff[layer, c] for c in range(4)]
    old_re, old_im = [state[layer, c].reshape(own, groups, states) for c in range(2)]
    new_re = decay_re * old_re - decay_im * old_im + weight_re * drive_re - weight_im * drive_im
    new_im = decay_re * old_im + decay_im * old_re + weight_re * drive_im + weight_im * drive_re
    value = jnp.einsum("bgp,gcp->bgc", new_re, n[layer, 0], precision=exact)
    value = value - jnp.einsum("bgp,gcp->bgc", new_im, n[layer, 1], precision=exact)
    value = value + skip[layer].reshape(groups, -1) * driven
    readout = jax.nn.gelu(value).reshape(own, -1).astype(BF16)
    new = jnp.stack([new_re, new_im]).reshape(1, 2, own, groups * states)
    if layer > 0:
        return readout, jnp.concatenate([so_far, new])
    chunk = feats // (inner * outer)
    start = lax.axis_index("tp") * chunk
    cuts = [lax.dynamic_slice_in_dim(p, start, chunk, axis=1) for p in pieces]
    return readout, new, jnp.concatenate(cuts, axis=1)


def plain_products(layer, dims, readout, weights):
    dp, inner, outer, model, own, feats = dims
    terms = []
    for w in weights:
        term = jnp.dot(readout, w[layer], preferred_element_type=F32)
        terms.append(term.reshape(own, outer, inner, -1))
    terms = jnp.concatenate(terms, axis=3).transpose(2, 1, 0, 3)
    low, _ = digits(inner)
    outs = [terms[low ^ k] for k in range(inner)]
    return [outs[0]] + [o.astype(BF16) for o in outs[1:]]


def plain_fold(value, arrived):
    for a in arrived:
        value = value + a.astype(F32)
    _, high = digits(len(arrived) + 1)
    outs = [value[high ^ k] for k in range(value.shape[0])]
    return [outs[0]] + [o.astype(BF16) for o in outs[1:]]


def plain_update(block, arrived, before):
    for a in arrived:
        block = block + a.astype(F32)
    half = block.shape[1] // 2
    gated = block[:, :half] * jax.nn.sigmoid(block[:, half:])
    return (before.astype(F32) + gated).astype(BF16)


def plain_settle(pieces, feats):
    rows = plain_order(pieces, len(pieces), pieces[0].shape[0])
    return rows.transpose(1, 0, 2).reshape(rows.shape[1], feats)


def make_body(tp, dp):
    inner = 1 << (int(math.log2(tp)) // 2)
    outer = tp // inner

    def body(
        tokens,
        lengths,
        norm_gain,
        w_in,
        log_step,
        eig_re,
        eig_im,
        in_mat,
        output_matrices,
        skip,
        w_glu,
        w_gate,
        state,
    ):
        layers = w_in.shape[0]
        seqs, feats = tokens.shape
        own = seqs // dp
        chunk = feats // tp
        dims = (dp, inner, outer, feats * dp, own, feats)
        me = lax.axis_index("dp")
        if chunk % 128 == 0 and own % 16 == 0 and skip.shape[1] % 128 == 0:
            stages = (prepare, recur, products, fold, update, settle)
        else:
            stages = (
                plain_prepare,
                plain_recur,
                plain_products,
                plain_fold,
                plain_update,
                plain_settle,
            )
        do_prepare, do_recur, do_products, do_fold, do_update, do_settle = stages

        def slabs(value):
            return [value] + [exchange(value, "dp", dp, 1, dp, k) for k in range(1, dp)]

        def over_low(value, k):
            return exchange(value, "tp", tp, 1, inner, k)

        def over_high(value, k):
            return exchange(value, "tp", tp, inner, outer, k)

        pieces = slabs(tokens)
        gain_slabs = slabs(norm_gain)
        in_slabs = slabs(w_in)
        glu_slabs = slabs(w_glu)
        gate_slabs = slabs(w_gate)
        coeff, m, n = do_prepare(lengths, log_step, eig_re, eig_im, in_mat, output_matrices)
        new_state = None
        for layer in range(layers):
            made = do_recur(
                layer, dims, pieces, gain_slabs, in_slabs, coeff, m, n, skip, state, new_state
            )
            readout, new_state = made[:2]
            if layer == 0:
                before = made[2]
            sends = do_products(layer, dims, readout, glu_slabs + gate_slabs)
            arrived = [over_low(sends[k], k) for k in range(1, inner)]
            sends = do_fold(sends[0], arrived)
            arrived = [over_high(sends[k], k) for k in range(1, outer)]
            shard = do_update(sends[0], arrived, before)
            before = shard
            if layer + 1 == layers:
                cuts = [shard[:, k * chunk : (k + 1) * chunk] for k in range(dp)]
                here = jnp.stack(
                    [cuts[0]] + [exchange(cuts[k], "dp", dp, 1, dp, k) for k in range(1, dp)]
                )
                if dp == 2:
                    flip = me == 1
                    shard = jnp.concatenate(
                        [jnp.where(flip, here[1], here[0]), jnp.where(flip, here[0], here[1])]
                    )
                else:
                    shard = here[me ^ jnp.arange(dp)].reshape(seqs, chunk)
            column = jnp.stack([shard] + [over_high(shard, k) for k in range(1, outer)])
            pieces = [column] + [over_low(column, k) for k in range(1, inner)]
        return (do_settle(pieces, feats), new_state)

    return body


def solution(mesh):
    placed = (
        P(None, "dp"),
        P("dp"),
        P(None, "dp"),
        P(None, "dp", "tp"),
        P(None, "tp"),
        P(None, "tp", None),
        P(None, "tp", None),
        P(None, None, "tp", None, None),
        P(None, None, "tp", None, None),
        P(None, "tp"),
        P(None, "tp", "dp"),
        P(None, "tp", "dp"),
        P(None, None, "dp", "tp"),
    )
    return jax.shard_map(
        make_body(mesh.shape["tp"], mesh.shape["dp"]),
        mesh=mesh,
        in_specs=placed,
        out_specs=(P(None, "dp"), P(None, None, "dp", "tp")),
        check_vma=False,
    )
```

```python
import functools
import math

import jax
import jax.numpy as jnp
from jax import lax
from jax.experimental import pallas as pl
from jax.experimental.pallas import tpu as pltpu
from jax.sharding import PartitionSpec as P


BLOCK_LEN = 256
LEN_MAX = 4096
NORM_EPS = 1e-06
F32 = jnp.float32
BF16 = jnp.bfloat16


def position_factor(lengths):
    blocks = (lengths // BLOCK_LEN).astype(F32)
    return 2.0 / (1.0 + blocks * (4.0 * BLOCK_LEN / LEN_MAX))


def exchange(value, axis, size, stride, count, k):
    pairs = []
    for i in range(size):
        digit = (i // stride) % count
        pairs.append((i, i + ((digit ^ k) - digit) * stride))
    return lax.ppermute(value, axis, pairs)


def params(mib=16):
    return pltpu.CompilerParams(vmem_limit_bytes=mib << 20)


VMEM = pl.BlockSpec(memory_space=pltpu.VMEM)
ANY = pl.BlockSpec(memory_space=pl.ANY)
HBM = pl.BlockSpec(memory_space=pltpu.HBM)


def struct(shape, dtype):
    return jax.ShapeDtypeStruct(shape, dtype)


def nt_dot(a, b):
    return lax.dot_general(a, b, (((1,), (1,)), ((), ())), preferred_element_type=F32)


def digits(inner):
    index = lax.axis_index("tp")
    return index % inner, index // inner


def corner():
    index = lax.axis_index("tp")
    return index % 4, (index // 4) % 2, index // 8


def placed_pieces(pieces, chunk):
    low, near, _ = corner()
    for k in range(4):
        for j in range(2):
            for far in range(2):
                at = ((2 * far + (near ^ j)) * 4 + (low ^ k)) * chunk
                yield pl.multiple_of(at, chunk), pieces[k][j, far]


def iota(shape, axis):
    return lax.broadcasted_iota(jnp.int32, shape, axis)


def exact_dot(a, b):
    return jnp.dot(a, b, precision=lax.Precision.HIGHEST, preferred_element_type=F32)


def prepare_kernel(count, *refs):
    lengths_ref, step_ref, re_ref, im_ref, in_ref, out_ref = refs[:6]
    stacks, (coeff_ref, m_ref, n_ref) = refs[6 : 6 + count], refs[6 + count : 9 + count]
    copies = [
        pltpu.make_async_copy(stacks[i].at[1], refs[9 + count + i], refs[-1].at[i])
        for i in range(count)
    ]
    for copy in copies:
        copy.start()
    layers, groups, states = re_ref.shape
    total, width = coeff_ref.shape[3], n_ref.shape[2]
    group = width // groups
    own = lengths_ref.shape[1]
    row = jnp.broadcast_to(position_factor(lengths_ref[...]), (own, own))
    factor = jnp.sum(
        jnp.where(iota((own, own), 0) == iota((own, own), 1), row, 0.0), axis=1, keepdims=True
    )
    spread = (iota((states, total), 1) % states == iota((states, total), 0)).astype(F32)
    spread_half = spread.astype(BF16)
    of_group = iota((groups, total), 1) // states == iota((groups, total), 0)
    keep = iota((width, total), 0) // group == iota((width, total), 1) // states

    def flat(value):
        return jnp.sum(
            jnp.where(of_group, exact_dot(value, spread), 0.0), axis=0, keepdims=True
        )

    for layer in range(layers):
        log_step = exact_dot(step_ref[layer : layer + 1, :], of_group.astype(F32))
        eig_re = flat(re_ref[layer])
        eig_im = flat(im_ref[layer])
        step_size = jnp.exp(log_step) * factor
        magnitude = jnp.exp(eig_re * step_size)
        turned = eig_im * step_size
        decay_re = magnitude * jnp.cos(turned)
        decay_im = magnitude * jnp.sin(turned)
        scale = 1.0 / (eig_re * eig_re + eig_im * eig_im)
        coeff_ref[layer, 0] = decay_re
        coeff_ref[layer, 1] = decay_im
        coeff_ref[layer, 2] = ((decay_re - 1.0) * eig_re + decay_im * eig_im) * scale
        coeff_ref[layer, 3] = (decay_im * eig_re - (decay_re - 1.0) * eig_im) * scale
        for part in range(2):
            for source, target in ((in_ref, m_ref), (out_ref, n_ref)):
                value = jnp.dot(
                    source[layer, part].astype(BF16), spread_half, preferred_element_type=F32
                )
                if part == 1 and target is n_ref:
                    value = -value
                target[layer, part] = jnp.where(keep, value, 0.0).astype(BF16)
    for copy in copies:
        copy.wait()


def prepare(own, lengths, log_step, eig_re, eig_im, in_rows, out_rows, stacks):
    layers, groups, states = eig_re.shape
    total, width = groups * states, in_rows.shape[2]
    outs = [
        struct((layers, 4, own, total), F32),
        struct((layers, 2, width, total), BF16),
        struct((layers, 2, width, total), BF16),
    ] + [pltpu.VMEM(a.shape[1:], a.dtype) for a in stacks]
    args = [lengths, log_step, eig_re, eig_im, in_rows, out_rows]
    specs = [VMEM] * len(args) + [HBM] * len(stacks)
    args += [pltpu.with_memory_space_constraint(a, pltpu.HBM) for a in stacks]
    made = pl.pallas_call(
        functools.partial(prepare_kernel, len(stacks)),
        in_specs=specs,
        out_specs=[VMEM] * len(outs),
        out_shape=outs,
        scratch_shapes=[pltpu.SemaphoreType.DMA((len(stacks),))],
        compiler_params=params(4),
        cost_estimate=pl.CostEstimate(flops=8 << 20, bytes_accessed=3 << 20, transcendentals=0),
        name="prepare",
    )(*args)
    return made[:3], made[3:]


def project_kernel(count, *refs):
    tokens_hbm, gain_hbm, weight_hbm = refs[:3]
    sources, (keep, send), targets = refs[3 : 3 + count], refs[3 + count : 5 + count], refs[5 + count : -4]
    tokens, gain, weight, sems = refs[-4:]
    pairs = [(tokens_hbm, tokens), (gain_hbm, gain), (weight_hbm.at[0], weight)]
    pairs += [(a.at[0] if len(a.shape) > len(b.shape) else a, b) for a, b in zip(sources, targets)]
    copies = [pltpu.make_async_copy(a, b, sems.at[i]) for i, (a, b) in enumerate(pairs)]
    for copy in copies:
        copy.start()
    own, width = keep.shape[0], weight.shape[1]
    chunk = tokens.shape[1] // 16
    copies[0].wait()
    copies[1].wait()
    current = tokens[...].astype(F32)
    squares = jnp.sum(current * current, axis=1, keepdims=True)
    scaled = (current * gain[0:1, :]).astype(BF16)
    copies[2].wait()
    term = jnp.dot(scaled, weight[...], preferred_element_type=F32)
    low, near, _ = corner()
    me = lax.axis_index("dp")
    for out, flip in ((keep, me), (send, 1 - me)):
        upper = flip == 1
        out[:, :width] = jnp.where(upper, term[own:], term[:own])
        out[:, width : width + 128] = jnp.broadcast_to(
            jnp.where(upper, squares[own:], squares[:own]), (own, 128)
        )
        start = pl.multiple_of(flip * own, own)
        for far in range(2):
            at = pl.multiple_of(((2 * far + near) * 4 + low) * chunk, chunk)
            base = width + 128 + far * chunk
            out[:, base : base + chunk] = tokens[pl.ds(start, own), pl.ds(at, chunk)].astype(F32)
    for copy in copies[3:]:
        copy.wait()


def project(dims, tokens, gain, weight, others, stacks):
    _, _, _, _, own, feats = dims
    width = weight.shape[2]
    shape = (own, width + 128 + 2 * feats // 16)
    args = [pltpu.with_memory_space_constraint(a, pltpu.HBM) for a in (tokens, gain, weight, *others, *stacks)]
    made = pl.pallas_call(
        functools.partial(project_kernel, len(others) + len(stacks)),
        in_specs=[HBM] * len(args),
        out_specs=[VMEM] * (2 + len(others) + len(stacks)),
        out_shape=[struct(shape, F32)] * 2 + [pltpu.VMEM(a.shape, a.dtype) for a in others]
        + [pltpu.VMEM(a.shape[1:], a.dtype) for a in stacks],
        scratch_shapes=[
            pltpu.VMEM(tokens.shape, BF16),
            pltpu.VMEM(gain.shape, F32),
            pltpu.VMEM(weight.shape[1:], BF16),
            pltpu.SemaphoreType.DMA((len(args),)),
        ],
        compiler_params=params(4),
        cost_estimate=pl.CostEstimate(flops=32 << 20, bytes_accessed=1 << 20, transcendentals=0),
        name="project",
    )(*args)
    return made[0], made[1], made[2 : 2 + len(others)], made[2 + len(others) :]


def recur_kernel(layer, dp, model, n_pieces, *refs):
    coeff_ref, m_ref, n_ref, skip_ref, state_ref = refs[:5]
    pieces = refs[5 : 5 + n_pieces]
    line, new_ref, sem = refs[-3:]
    own, feats = line.shape[1:]
    width = skip_ref.shape[1]
    chunk = feats // 16
    if layer == 0:
        readout_ref, state_out, before_ref = refs[-6:-3]
        partial_value = pieces[0][:, :width] + pieces[1][:, :width]
        squares = (pieces[0][:, width : width + 128] + pieces[1][:, width : width + 128])[:, :1]
        for far in range(2):
            for p in range(dp):
                base = width + 128 + far * chunk
                before_ref[far, :, p * chunk : (p + 1) * chunk] = pieces[p][
                    :, base : base + chunk
                ].astype(BF16)
    else:
        readout_ref, state_out = refs[-5:-3]
        gains = refs[5 + n_pieces : 5 + n_pieces + dp]
        weights = refs[5 + n_pieces + dp : 5 + n_pieces + 2 * dp]
        for at, piece in placed_pieces(pieces, chunk):
            for p in range(dp):
                line[p, :, pl.ds(at, chunk)] = piece[:, p * chunk : (p + 1) * chunk]
        squares = jnp.zeros((own, 1), F32)
        partial_value = None
        for p in range(dp):
            current = line[p].astype(F32)
            squares = squares + jnp.sum(current * current, axis=1, keepdims=True)
            scaled = (current * gains[p][layer : layer + 1, :]).astype(BF16)
            term = jnp.dot(scaled, weights[p][...], preferred_element_type=F32)
            partial_value = term if partial_value is None else partial_value + term
    driven = (partial_value * lax.rsqrt(squares / model + NORM_EPS)).astype(BF16)
    drive_re = jnp.dot(driven, m_ref[layer, 0], preferred_element_type=F32)
    drive_im = jnp.dot(driven, m_ref[layer, 1], preferred_element_type=F32)
    decay_re, decay_im = coeff_ref[layer, 0], coeff_ref[layer, 1]
    weight_re, weight_im = coeff_ref[layer, 2], coeff_ref[layer, 3]
    old_re, old_im = state_ref[layer, 0], state_ref[layer, 1]
    new_re = decay_re * old_re - decay_im * old_im + weight_re * drive_re - weight_im * drive_im
    new_im = decay_re * old_im + decay_im * old_re + weight_re * drive_im + weight_im * drive_re
    new_ref[0] = new_re
    new_ref[1] = new_im
    copy = pltpu.make_async_copy(new_ref, state_out.at[layer], sem)
    copy.start()
    value = nt_dot(new_re.astype(BF16), n_ref[layer, 0])
    value = value + nt_dot(new_im.astype(BF16), n_ref[layer, 1])
    value = value + skip_ref[layer : layer + 1, :] * driven.astype(F32)
    readout_ref[...] = jax.nn.gelu(value).astype(BF16)
    copy.wait()


def recur(layer, dims, consts, pieces, slabs, so_far):
    dp, _, _, model, own, feats = dims
    skip, state = consts[3:]
    args = [*consts, *pieces, *slabs]
    specs = [VMEM] * len(args)
    outs = [struct((own, skip.shape[1]), BF16), struct(state.shape, F32)]
    out_specs = [VMEM, ANY]
    alias = {}
    if layer == 0:
        outs.append(struct((2, own, dp * feats // 16), BF16))
        out_specs.append(VMEM)
    else:
        alias = {len(args): 1}
        args.append(so_far)
        specs.append(ANY)
    return pl.pallas_call(
        functools.partial(recur_kernel, layer, dp, model, len(pieces)),
        in_specs=specs,
        out_specs=out_specs,
        out_shape=outs,
        scratch_shapes=[
            pltpu.VMEM((dp, own, feats), BF16),
            pltpu.VMEM(state.shape[1:], F32),
            pltpu.SemaphoreType.DMA,
        ],
        input_output_aliases=alias,
        compiler_params=params(8),
        cost_estimate=pl.CostEstimate(flops=64 << 20, bytes_accessed=2 << 20, transcendentals=0),
    )(*args)


def product_kernel(chunk, readout_ref, *refs):
    weights, outs, spread = refs[:-5], refs[-5:-1], refs[-1]
    count = len(weights)
    low, _, _ = corner()
    readout = readout_ref[...]
    for w in range(count):
        value = jnp.dot(readout, weights[w][...], preferred_element_type=F32)
        for j in range(16):
            spread[w, j] = value[:, j * chunk : (j + 1) * chunk]
    for k in range(4):
        for h in range(4):
            for w in range(count):
                outs[k][h, :, w * chunk : (w + 1) * chunk] = spread[w, h * 4 + (low ^ k)].astype(
                    outs[k].dtype
                )


def call(kernel, args, outs, scratch=(), mib=4):
    return pl.pallas_call(
        kernel,
        in_specs=[VMEM] * len(args),
        out_specs=[VMEM] * len(outs),
        out_shape=outs,
        scratch_shapes=scratch,
        compiler_params=params(mib),
        cost_estimate=pl.CostEstimate(flops=1 << 22, bytes_accessed=1 << 20, transcendentals=0),
    )(*args)


def products(dims, readout, weights):
    _, _, _, _, own, feats = dims
    chunk = feats // 16
    shape = (4, own, len(weights) * chunk)
    return call(
        functools.partial(product_kernel, chunk),
        (readout, *weights),
        [struct(shape, F32)] + [struct(shape, BF16)] * 3,
        [pltpu.VMEM((len(weights), 16, own, chunk), F32)],
        8,
    )


def fold_low_kernel(own_ref, a_ref, b_ref, c_ref, keep, send):
    _, near, _ = corner()
    for far in range(2):
        for out, turn in ((keep, 0), (send, 1)):
            at = 2 * far + (near ^ turn)
            total = own_ref[at] + a_ref[at].astype(F32) + b_ref[at].astype(F32)
            out[far] = (total + c_ref[at].astype(F32)).astype(out.dtype)


def fold_near_kernel(own_ref, arrived_ref, send):
    send[...] = (own_ref[...] + arrived_ref[...].astype(F32)).astype(BF16)


def updated(own_ref, arrived_ref, before_ref):
    total = own_ref[...].astype(F32) + arrived_ref[...].astype(F32)
    half = total.shape[2] // 2
    linear, gate = total[:, :, :half], total[:, :, half:]
    return (before_ref[...].astype(F32) + linear * jax.nn.sigmoid(gate)).astype(BF16)


def update_kernel(own_ref, arrived_ref, before_ref, out):
    out[...] = updated(own_ref, arrived_ref, before_ref)


def last_update_kernel(own_ref, arrived_ref, before_ref, keep, send):
    value = updated(own_ref, arrived_ref, before_ref)
    half = value.shape[2] // 2
    keep[...] = value[:, :, :half]
    send[...] = value[:, :, half:]


def merge_kernel(own_ref, arrived_ref, out):
    rows = own_ref.shape[1]
    me = lax.axis_index("dp")
    out[:, pl.ds(pl.multiple_of(me * rows, rows), rows), :] = own_ref[...]
    out[:, pl.ds(pl.multiple_of((1 - me) * rows, rows), rows), :] = arrived_ref[...]


def settle_kernel(chunk, *refs):
    pieces, out, sem = refs[:4], refs[4], refs[5]
    copies = []
    for i, (at, _) in enumerate(placed_pieces(pieces, chunk)):
        source = pieces[i // 4].at[(i // 2) % 2, i % 2]
        copies.append(pltpu.make_async_copy(source, out.at[:, pl.ds(at, chunk)], sem.at[i]))
        copies[-1].start()
    for copy in copies:
        copy.wait()


def settle(pieces, feats):
    rows, chunk = pieces[0].shape[2:]
    return pl.pallas_call(
        functools.partial(settle_kernel, chunk),
        in_specs=[VMEM] * 4,
        out_specs=ANY,
        out_shape=struct((rows, feats), BF16),
        scratch_shapes=[pltpu.SemaphoreType.DMA((16,))],
        compiler_params=params(4),
        name="settle",
    )(*pieces)


def plain_prepare(lengths, log_step, eig_re, eig_im, in_mat, output_matrices):
    factor = position_factor(lengths)
    step_size = jnp.exp(log_step)[:, None, :, None] * factor[None, :, None, None]
    eig_re, eig_im = eig_re[:, None], eig_im[:, None]
    magnitude = jnp.exp(eig_re * step_size)
    turned = eig_im * step_size
    decay_re = magnitude * jnp.cos(turned)
    decay_im = magnitude * jnp.sin(turned)
    modulus = eig_re * eig_re + eig_im * eig_im
    weight_re = ((decay_re - 1.0) * eig_re + decay_im * eig_im) / modulus
    weight_im = (decay_im * eig_re - (decay_re - 1.0) * eig_im) / modulus
    return jnp.stack([decay_re, decay_im, weight_re, weight_im], axis=1), in_mat, output_matrices


def plain_order(pieces, inner, outer):
    low, high = digits(inner)
    rows = []
    for h in range(outer):
        for l in range(inner):
            row = jnp.stack(pieces)[low ^ l, high ^ h]
            rows.append(row)
    return jnp.stack(rows)


def plain_recur(layer, dims, pieces, gains, weights, coeff, m, n, skip, state, so_far):
    dp, inner, outer, model, own, feats = dims
    groups, states = coeff.shape[3:]
    if layer > 0:
        rows = plain_order(pieces, inner, outer)
        rows = rows.reshape(inner * outer, own, dp, feats // (inner * outer))
        pieces = [rows[:, :, p].transpose(1, 0, 2).reshape(own, feats) for p in range(dp)]
    else:
        start = lax.axis_index("dp") * own
        pieces = [lax.dynamic_slice_in_dim(p, start, own, axis=0) for p in pieces]
    squares, partial_value = 0.0, 0.0
    for p in range(dp):
        current = pieces[p].astype(F32)
        squares = squares + jnp.sum(current * current, axis=1, keepdims=True)
        scaled = (current * gains[p][layer]).astype(BF16)
        partial_value = partial_value + jnp.dot(
            scaled, weights[p][layer], preferred_element_type=F32
        )
    driven = (partial_value * lax.rsqrt(squares / model + NORM_EPS)).astype(BF16).astype(F32)
    driven = driven.reshape(own, groups, -1)
    exact = lax.Precision.HIGHEST
    drive_re = jnp.einsum("bgc,gpc->bgp", driven, m[layer, 0], precision=exact)
    drive_im = jnp.einsum("bgc,gpc->bgp", driven, m[layer, 1], precision=exact)
    decay_re, decay_im, weight_re, weight_im = [coeff[layer, c] for c in range(4)]
    old_re, old_im = [state[layer, c].reshape(own, groups, states) for c in range(2)]
    new_re = decay_re * old_re - decay_im * old_im + weight_re * drive_re - weight_im * drive_im
    new_im = decay_re * old_im + decay_im * old_re + weight_re * drive_im + weight_im * drive_re
    value = jnp.einsum("bgp,gcp->bgc", new_re, n[layer, 0], precision=exact)
    value = value - jnp.einsum("bgp,gcp->bgc", new_im, n[layer, 1], precision=exact)
    value = value + skip[layer].reshape(groups, -1) * driven
    readout = jax.nn.gelu(value).reshape(own, -1).astype(BF16)
    new = jnp.stack([new_re, new_im]).reshape(1, 2, own, groups * states)
    if layer > 0:
        return readout, jnp.concatenate([so_far, new])
    chunk = feats // (inner * outer)
    start = lax.axis_index("tp") * chunk
    cuts = [lax.dynamic_slice_in_dim(p, start, chunk, axis=1) for p in pieces]
    return readout, new, jnp.concatenate(cuts, axis=1)


def plain_products(layer, dims, readout, weights):
    _, inner, outer, _, own, _ = dims
    terms = []
    for w in weights:
        term = jnp.dot(readout, w[layer], preferred_element_type=F32)
        terms.append(term.reshape(own, outer, inner, -1))
    terms = jnp.concatenate(terms, axis=3).transpose(2, 1, 0, 3)
    low, _ = digits(inner)
    outs = [terms[low ^ k] for k in range(inner)]
    return [outs[0]] + [o.astype(BF16) for o in outs[1:]]


def plain_fold(value, arrived):
    for a in arrived:
        value = value + a.astype(F32)
    _, high = digits(len(arrived) + 1)
    outs = [value[high ^ k] for k in range(value.shape[0])]
    return [outs[0]] + [o.astype(BF16) for o in outs[1:]]


def plain_update(block, arrived, before):
    for a in arrived:
        block = block + a.astype(F32)
    half = block.shape[1] // 2
    gated = block[:, :half] * jax.nn.sigmoid(block[:, half:])
    return (before.astype(F32) + gated).astype(BF16)


def plain_settle(pieces, feats):
    rows = plain_order(pieces, len(pieces), pieces[0].shape[0])
    return rows.transpose(1, 0, 2).reshape(rows.shape[1], feats)


def plain_layers(dims, layers, pieces, slabs_of, pointwise):
    dp, inner, outer, _, own, feats = dims
    gain_slabs, in_slabs, out_slabs = slabs_of
    lengths, log_step, eig_re, eig_im, in_mat, output_matrices, skip, state = pointwise
    tp = inner * outer
    chunk = feats // tp

    def over_low(value, k):
        return exchange(value, "tp", tp, 1, inner, k)

    def over_high(value, k):
        return exchange(value, "tp", tp, inner, outer, k)

    coeff, m, n = plain_prepare(lengths, log_step, eig_re, eig_im, in_mat, output_matrices)
    new_state = None
    for layer in range(layers):
        made = plain_recur(
            layer, dims, pieces, gain_slabs, in_slabs, coeff, m, n, skip, state, new_state
        )
        readout, new_state = made[:2]
        if layer == 0:
            before = made[2]
        sends = plain_products(layer, dims, readout, out_slabs)
        arrived = [over_low(sends[k], k) for k in range(1, inner)]
        sends = plain_fold(sends[0], arrived)
        arrived = [over_high(sends[k], k) for k in range(1, outer)]
        shard = plain_update(sends[0], arrived, before)
        before = shard
        if layer + 1 == layers:
            cuts = [shard[:, k * chunk : (k + 1) * chunk] for k in range(dp)]
            here = [cuts[0]] + [exchange(cuts[k], "dp", dp, 1, dp, k) for k in range(1, dp)]
            order = lax.axis_index("dp") ^ jnp.arange(dp)
            shard = jnp.stack(here)[order].reshape(own * dp, chunk)
        column = jnp.stack([shard] + [over_high(shard, k) for k in range(1, outer)])
        pieces = [column] + [over_low(column, k) for k in range(1, inner)]
    return plain_settle(pieces, feats), new_state


def kernel_layers(dims, tokens, norm_gain, w_in, w_glu, w_gate, pointwise):
    dp, _, _, _, own, feats = dims
    lengths, log_step, eig_re, eig_im, in_mat, output_matrices, skip, state = pointwise
    layers = w_in.shape[0]
    chunk = feats // 16
    wide = 2 * dp * chunk

    def core_swap(value):
        return exchange(value, "dp", 2, 1, 2, 1)

    def over_low(value, k):
        return exchange(value, "tp", 16, 1, 4, k)

    def over_near(value):
        return exchange(value, "tp", 16, 4, 2, 1)

    def over_far(value):
        return exchange(value, "tp", 16, 8, 2, 1)

    width = skip.shape[1]
    others = (
        lengths[None, :],
        log_step,
        eig_re,
        eig_im,
        jnp.swapaxes(in_mat, 3, 4).reshape(layers, 2, width, -1),
        output_matrices.reshape(layers, 2, width, -1),
        skip,
        state,
    )
    keep, send, others, outward = project(
        dims, tokens, norm_gain, w_in, others, (w_glu, w_gate)
    )
    pieces = [keep, core_swap(send)]
    outward = [outward[0], core_swap(outward[0]), outward[1], core_swap(outward[1])]
    made, later = prepare(own, *others[:6], (w_in, w_glu, w_gate))
    consts = (*made, *others[6:])
    slabs = []
    new_state = None
    for layer in range(layers):
        made = recur(layer, dims, consts, pieces, slabs, new_state)
        readout, new_state = made[:2]
        if layer == 0:
            before = made[2]
        parts = products(dims, readout, outward)
        arrived = [over_low(parts[k], k) for k in range(1, 4)]
        if layer + 1 < layers:
            *later, gain, _ = lax.optimization_barrier((*later, norm_gain, parts[0]))
            slabs = [norm_gain, core_swap(gain), later[0], core_swap(later[0])]
            outward = [later[1], core_swap(later[1]), later[2], core_swap(later[2])]
        keep, send = call(
            fold_low_kernel,
            (parts[0], *arrived),
            [struct((2, own, wide), F32), struct((2, own, wide), BF16)],
        )
        (send,) = call(fold_near_kernel, (keep, over_near(send)), [struct((2, own, wide), BF16)])
        terms = (send, over_far(send), before)
        if layer + 1 < layers:
            (shard,) = call(update_kernel, terms, [struct((2, own, dp * chunk), BF16)])
            before = shard
        else:
            keep, send = call(last_update_kernel, terms, [struct((2, own, chunk), BF16)] * 2)
            (shard,) = call(
                merge_kernel, (keep, core_swap(send)), [struct((2, own * 2, chunk), BF16)]
            )
        column = jnp.stack([shard, over_near(shard)])
        pieces = [column] + [over_low(column, k) for k in range(1, 4)]
    return settle(pieces, feats), new_state


def make_body(tp, dp):
    inner = 1 << (int(math.log2(tp)) // 2)
    outer = tp // inner

    def body(
        tokens,
        lengths,
        norm_gain,
        w_in,
        log_step,
        eig_re,
        eig_im,
        in_mat,
        output_matrices,
        skip,
        w_glu,
        w_gate,
        state,
    ):
        layers = w_in.shape[0]
        seqs, feats = tokens.shape
        own = seqs // dp
        chunk = feats // tp
        dims = (dp, inner, outer, feats * dp, own, feats)
        pointwise = (lengths, log_step, eig_re, eig_im, in_mat, output_matrices, skip, state)
        regular = tp == 16 and dp == 2 and chunk % 128 == 0 and own % 16 == 0
        if regular and skip.shape[1] % 128 == 0:
            return kernel_layers(dims, tokens, norm_gain, w_in, w_glu, w_gate, pointwise)

        def slabs(value):
            return [value] + [exchange(value, "dp", dp, 1, dp, k) for k in range(1, dp)]

        slabs_of = (slabs(norm_gain), slabs(w_in), slabs(w_glu) + slabs(w_gate))
        return plain_layers(dims, layers, slabs(tokens), slabs_of, pointwise)

    return body


def solution(mesh):
    placed = (
        P(None, "dp"),
        P("dp"),
        P(None, "dp"),
        P(None, "dp", "tp"),
        P(None, "tp"),
        P(None, "tp", None),
        P(None, "tp", None),
        P(None, None, "tp", None, None),
        P(None, None, "tp", None, None),
        P(None, "tp"),
        P(None, "tp", "dp"),
        P(None, "tp", "dp"),
        P(None, None, "dp", "tp"),
    )
    return jax.shard_map(
        make_body(mesh.shape["tp"], mesh.shape["dp"]),
        mesh=mesh,
        in_specs=placed,
        out_specs=(P(None, "dp"), P(None, None, "dp", "tp")),
        check_vma=False,
    )
```

```python
import functools
import math

import jax
import jax.numpy as jnp
from jax import lax
from jax.experimental import pallas as pl
from jax.experimental.pallas import tpu as pltpu
from jax.sharding import PartitionSpec as P


BLOCK_LEN = 256
LEN_MAX = 4096
NORM_EPS = 1e-06
F32 = jnp.float32
BF16 = jnp.bfloat16


def position_factor(lengths):
    blocks = (lengths // BLOCK_LEN).astype(F32)
    return 2.0 / (1.0 + blocks * (4.0 * BLOCK_LEN / LEN_MAX))


def exchange(value, axis, size, stride, count, k):
    pairs = []
    for i in range(size):
        digit = (i // stride) % count
        pairs.append((i, i + ((digit ^ k) - digit) * stride))
    return lax.ppermute(value, axis, pairs)


def params(mib=16):
    return pltpu.CompilerParams(vmem_limit_bytes=mib << 20)


VMEM = pl.BlockSpec(memory_space=pltpu.VMEM)
ANY = pl.BlockSpec(memory_space=pl.ANY)
HBM = pl.BlockSpec(memory_space=pltpu.HBM)


def struct(shape, dtype):
    return jax.ShapeDtypeStruct(shape, dtype)


def nt_dot(a, b):
    return lax.dot_general(a, b, (((1,), (1,)), ((), ())), preferred_element_type=F32)


def digits(inner):
    index = lax.axis_index("tp")
    return index % inner, index // inner


def call(kernel, args, outs, scratch=(), mib=4):
    return pl.pallas_call(
        kernel,
        in_specs=[VMEM] * len(args),
        out_specs=[VMEM] * len(outs),
        out_shape=outs,
        scratch_shapes=scratch,
        compiler_params=params(mib),
        cost_estimate=pl.CostEstimate(flops=1 << 22, bytes_accessed=1 << 20, transcendentals=0),
    )(*args)


def corner():
    index = lax.axis_index("tp")
    return index % 4, (index // 4) % 2, index // 8


def placed_pieces(pieces, chunk):
    low, near, _ = corner()
    for k in range(4):
        for j in range(2):
            for far in range(2):
                at = ((2 * far + (near ^ j)) * 4 + (low ^ k)) * chunk
                yield pl.multiple_of(at, chunk), pieces[k][j, far]


def iota(shape, axis):
    return lax.broadcasted_iota(jnp.int32, shape, axis)


def exact_dot(a, b):
    return jnp.dot(a, b, precision=lax.Precision.HIGHEST, preferred_element_type=F32)


def prepare_kernel(
    lengths_ref, step_ref, re_ref, im_ref, in_ref, out_ref, coeff_ref, m_ref, n_ref
):
    layers, groups, states = re_ref.shape
    total, width = coeff_ref.shape[3], n_ref.shape[2]
    group = width // groups
    own = lengths_ref.shape[1]
    row = jnp.broadcast_to(position_factor(lengths_ref[...]), (own, own))
    factor = jnp.sum(
        jnp.where(iota((own, own), 0) == iota((own, own), 1), row, 0.0), axis=1, keepdims=True
    )
    spread = (iota((states, total), 1) % states == iota((states, total), 0)).astype(F32)
    spread_half = spread.astype(BF16)
    of_group = iota((groups, total), 1) // states == iota((groups, total), 0)
    keep = iota((width, total), 0) // group == iota((width, total), 1) // states

    def flat(value):
        return jnp.sum(
            jnp.where(of_group, exact_dot(value, spread), 0.0), axis=0, keepdims=True
        )

    for layer in range(layers):
        log_step = exact_dot(step_ref[layer : layer + 1, :], of_group.astype(F32))
        eig_re = flat(re_ref[layer])
        eig_im = flat(im_ref[layer])
        step_size = jnp.exp(log_step) * factor
        magnitude = jnp.exp(eig_re * step_size)
        turned = eig_im * step_size
        decay_re = magnitude * jnp.cos(turned)
        decay_im = magnitude * jnp.sin(turned)
        scale = 1.0 / (eig_re * eig_re + eig_im * eig_im)
        coeff_ref[layer, 0] = decay_re
        coeff_ref[layer, 1] = decay_im
        coeff_ref[layer, 2] = ((decay_re - 1.0) * eig_re + decay_im * eig_im) * scale
        coeff_ref[layer, 3] = (decay_im * eig_re - (decay_re - 1.0) * eig_im) * scale
        for part in range(2):
            for source, target in ((in_ref, m_ref), (out_ref, n_ref)):
                value = jnp.dot(
                    source[layer, part].astype(BF16), spread_half, preferred_element_type=F32
                )
                if part == 1 and target is n_ref:
                    value = -value
                target[layer, part] = jnp.where(keep, value, 0.0).astype(BF16)


def prepare(own, lengths, log_step, eig_re, eig_im, in_rows, out_rows):
    layers, groups, states = eig_re.shape
    total, width = groups * states, in_rows.shape[2]
    outs = [
        struct((layers, 4, own, total), F32),
        struct((layers, 2, width, total), BF16),
        struct((layers, 2, width, total), BF16),
    ]
    args = (lengths, log_step, eig_re, eig_im, in_rows, out_rows)
    return call(prepare_kernel, args, outs)


def pack_kernel(in_hbm, glu_hbm, gate_hbm, in_out, *refs):
    packs, sem, sems = refs[:4], refs[4], refs[5]
    chunk = packs[0].shape[1] // 8
    low, _, _ = corner()
    copies = [pltpu.make_async_copy(in_hbm.at[1], in_out, sem)]
    for k in range(4):
        for w, source in enumerate((glu_hbm, gate_hbm)):
            for h in range(4):
                at = pl.multiple_of((h * 4 + (low ^ k)) * chunk, chunk)
                copies.append(
                    pltpu.make_async_copy(
                        source.at[1, :, pl.ds(at, chunk)],
                        packs[k].at[:, (w * 4 + h) * chunk : (w * 4 + h + 1) * chunk],
                        sems.at[k, w, h],
                    )
                )
    for copy in copies:
        copy.start()
    for copy in copies:
        copy.wait()


def pack(w_in, w_glu, w_gate):
    width, chunk = w_glu.shape[1], w_glu.shape[2] // 16
    args = [pltpu.with_memory_space_constraint(a, pltpu.HBM) for a in (w_in, w_glu, w_gate)]
    outs = [pltpu.VMEM(w_in.shape[1:], BF16)] + [pltpu.VMEM((width, 8 * chunk), BF16)] * 4
    return pl.pallas_call(
        pack_kernel,
        in_specs=[HBM] * 3,
        out_specs=[VMEM] * 5,
        out_shape=outs,
        scratch_shapes=[pltpu.SemaphoreType.DMA, pltpu.SemaphoreType.DMA((4, 2, 4))],
        compiler_params=params(4),
        cost_estimate=pl.CostEstimate(flops=8 << 20, bytes_accessed=3 << 20, transcendentals=0),
        name="pack",
    )(*args)


def project_kernel(count, *refs):
    tokens_hbm, gain_hbm, weight_hbm = refs[:3]
    sources, (keep, send), targets = refs[3 : 3 + count], refs[3 + count : 5 + count], refs[5 + count : -4]
    tokens, gain, weight, sems = refs[-4:]
    pairs = [(tokens_hbm, tokens), (gain_hbm, gain), (weight_hbm.at[0], weight)]
    pairs += [(a.at[0] if len(a.shape) > len(b.shape) else a, b) for a, b in zip(sources, targets)]
    copies = [pltpu.make_async_copy(a, b, sems.at[i]) for i, (a, b) in enumerate(pairs)]
    for copy in copies:
        copy.start()
    own, width = keep.shape[0], weight.shape[1]
    chunk = tokens.shape[1] // 16
    copies[0].wait()
    copies[1].wait()
    current = tokens[...].astype(F32)
    squares = jnp.sum(current * current, axis=1, keepdims=True)
    scaled = (current * gain[0:1, :]).astype(BF16)
    copies[2].wait()
    term = jnp.dot(scaled, weight[...], preferred_element_type=F32)
    low, near, _ = corner()
    me = lax.axis_index("dp")
    for out, flip in ((keep, me), (send, 1 - me)):
        upper = flip == 1
        out[:, :width] = jnp.where(upper, term[own:], term[:own])
        out[:, width : width + 128] = jnp.broadcast_to(
            jnp.where(upper, squares[own:], squares[:own]), (own, 128)
        )
        start = pl.multiple_of(flip * own, own)
        for far in range(2):
            at = pl.multiple_of(((2 * far + near) * 4 + low) * chunk, chunk)
            base = width + 128 + far * chunk
            out[:, base : base + chunk] = tokens[pl.ds(start, own), pl.ds(at, chunk)].astype(F32)
    for copy in copies[3:]:
        copy.wait()


def project(dims, tokens, gain, weight, others, stacks):
    _, _, _, _, own, feats = dims
    width = weight.shape[2]
    shape = (own, width + 128 + 2 * feats // 16)
    args = [pltpu.with_memory_space_constraint(a, pltpu.HBM) for a in (tokens, gain, weight, *others, *stacks)]
    made = pl.pallas_call(
        functools.partial(project_kernel, len(others) + len(stacks)),
        in_specs=[HBM] * len(args),
        out_specs=[VMEM] * (2 + len(others) + len(stacks)),
        out_shape=[struct(shape, F32)] * 2 + [pltpu.VMEM(a.shape, a.dtype) for a in others]
        + [pltpu.VMEM(a.shape[1:], a.dtype) for a in stacks],
        scratch_shapes=[
            pltpu.VMEM(tokens.shape, BF16),
            pltpu.VMEM(gain.shape, F32),
            pltpu.VMEM(weight.shape[1:], BF16),
            pltpu.SemaphoreType.DMA((len(args),)),
        ],
        compiler_params=params(4),
        cost_estimate=pl.CostEstimate(flops=32 << 20, bytes_accessed=1 << 20, transcendentals=0),
        name="project",
    )(*args)
    return made[0], made[1], made[2 : 2 + len(others)], made[2 + len(others) :]


def recur_kernel(layer, dp, model, n_pieces, *refs):
    coeff_ref, m_ref, n_ref, skip_ref, state_ref = refs[:5]
    pieces = refs[5 : 5 + n_pieces]
    line, new_ref, sem = refs[-3:]
    own, feats = line.shape[1:]
    width = skip_ref.shape[1]
    chunk = feats // 16
    if layer == 0:
        readout_ref, state_out, before_ref = refs[-6:-3]
        partial_value = pieces[0][:, :width] + pieces[1][:, :width]
        squares = (pieces[0][:, width : width + 128] + pieces[1][:, width : width + 128])[:, :1]
        for far in range(2):
            for p in range(dp):
                base = width + 128 + far * chunk
                before_ref[far, :, p * chunk : (p + 1) * chunk] = pieces[p][
                    :, base : base + chunk
                ].astype(BF16)
    else:
        readout_ref, state_out = refs[-5:-3]
        gains = refs[5 + n_pieces : 5 + n_pieces + dp]
        weights = refs[5 + n_pieces + dp : 5 + n_pieces + 2 * dp]
        for at, piece in placed_pieces(pieces, chunk):
            for p in range(dp):
                line[p, :, pl.ds(at, chunk)] = piece[:, p * chunk : (p + 1) * chunk]
        squares = jnp.zeros((own, 1), F32)
        partial_value = None
        for p in range(dp):
            current = line[p].astype(F32)
            squares = squares + jnp.sum(current * current, axis=1, keepdims=True)
            scaled = (current * gains[p][layer : layer + 1, :]).astype(BF16)
            term = jnp.dot(scaled, weights[p][...], preferred_element_type=F32)
            partial_value = term if partial_value is None else partial_value + term
    driven = (partial_value * lax.rsqrt(squares / model + NORM_EPS)).astype(BF16)
    drive_re = jnp.dot(driven, m_ref[layer, 0], preferred_element_type=F32)
    drive_im = jnp.dot(driven, m_ref[layer, 1], preferred_element_type=F32)
    decay_re, decay_im = coeff_ref[layer, 0], coeff_ref[layer, 1]
    weight_re, weight_im = coeff_ref[layer, 2], coeff_ref[layer, 3]
    old_re, old_im = state_ref[layer, 0], state_ref[layer, 1]
    new_re = decay_re * old_re - decay_im * old_im + weight_re * drive_re - weight_im * drive_im
    new_im = decay_re * old_im + decay_im * old_re + weight_re * drive_im + weight_im * drive_re
    new_ref[0] = new_re
    new_ref[1] = new_im
    copy = pltpu.make_async_copy(new_ref, state_out.at[layer], sem)
    copy.start()
    value = nt_dot(new_re.astype(BF16), n_ref[layer, 0])
    value = value + nt_dot(new_im.astype(BF16), n_ref[layer, 1])
    value = value + skip_ref[layer : layer + 1, :] * driven.astype(F32)
    readout_ref[...] = jax.nn.gelu(value).astype(BF16)
    copy.wait()


def recur(layer, dims, consts, pieces, slabs, so_far):
    dp, _, _, model, own, feats = dims
    skip, state = consts[3:]
    args = [*consts, *pieces, *slabs]
    specs = [VMEM] * len(args)
    outs = [struct((own, skip.shape[1]), BF16), struct(state.shape, F32)]
    out_specs = [VMEM, ANY]
    alias = {}
    if layer == 0:
        outs.append(struct((2, own, dp * feats // 16), BF16))
        out_specs.append(VMEM)
    else:
        alias = {len(args): 1}
        args.append(so_far)
        specs.append(ANY)
    return pl.pallas_call(
        functools.partial(recur_kernel, layer, dp, model, len(pieces)),
        in_specs=specs,
        out_specs=out_specs,
        out_shape=outs,
        scratch_shapes=[
            pltpu.VMEM((dp, own, feats), BF16),
            pltpu.VMEM(state.shape[1:], F32),
            pltpu.SemaphoreType.DMA,
        ],
        input_output_aliases=alias,
        compiler_params=params(8),
        cost_estimate=pl.CostEstimate(flops=64 << 20, bytes_accessed=2 << 20, transcendentals=0),
    )(*args)


def product_kernel(chunk, readout_ref, *refs):
    weights, outs, spread = refs[:-5], refs[-5:-1], refs[-1]
    count = len(weights)
    low, _, _ = corner()
    readout = readout_ref[...]
    for w in range(count):
        value = jnp.dot(readout, weights[w][...], preferred_element_type=F32)
        for j in range(16):
            spread[w, j] = value[:, j * chunk : (j + 1) * chunk]
    for k in range(4):
        for h in range(4):
            for w in range(count):
                outs[k][h, :, w * chunk : (w + 1) * chunk] = spread[w, h * 4 + (low ^ k)].astype(
                    outs[k].dtype
                )


def products(dims, readout, weights):
    _, _, _, _, own, feats = dims
    chunk = feats // 16
    shape = (4, own, len(weights) * chunk)
    return call(
        functools.partial(product_kernel, chunk),
        (readout, *weights),
        [struct(shape, F32)] + [struct(shape, BF16)] * 3,
        [pltpu.VMEM((len(weights), 16, own, chunk), F32)],
        8,
    )


def gathered_kernel(chunk, *refs):
    readouts, weights, (keep, send, spread) = refs[:4], refs[4:8], refs[8:]
    _, near, _ = corner()
    value = None
    for k in range(4):
        term = jnp.dot(readouts[k][...], weights[k][...], preferred_element_type=F32)
        value = term if value is None else value + term
    for j in range(8):
        spread[j] = value[:, j * chunk : (j + 1) * chunk]
    for far in range(2):
        for w in range(2):
            lanes = slice(w * chunk, (w + 1) * chunk)
            at = w * 4 + 2 * far + near
            keep[far, :, lanes] = spread[at]
            send[far, :, lanes] = spread[w * 4 + 2 * far + (near ^ 1)].astype(BF16)


def gathered_products(chunk, readouts, weights):
    rows = readouts[0].shape[0]
    return call(
        functools.partial(gathered_kernel, chunk),
        (*readouts, *weights),
        [struct((2, rows, 2 * chunk), F32), struct((2, rows, 2 * chunk), BF16)],
        [pltpu.VMEM((8, rows, chunk), F32)],
        8,
    )


def fold_low_kernel(own_ref, a_ref, b_ref, c_ref, keep, send):
    _, near, _ = corner()
    for far in range(2):
        for out, turn in ((keep, 0), (send, 1)):
            at = 2 * far + (near ^ turn)
            total = own_ref[at] + a_ref[at].astype(F32) + b_ref[at].astype(F32)
            out[far] = (total + c_ref[at].astype(F32)).astype(out.dtype)


def fold_near_kernel(own_ref, arrived_ref, send):
    send[...] = (own_ref[...] + arrived_ref[...].astype(F32)).astype(BF16)


def updated(own_ref, arrived_ref, before_ref):
    total = own_ref[...].astype(F32) + arrived_ref[...].astype(F32)
    half = total.shape[2] // 2
    linear, gate = total[:, :, :half], total[:, :, half:]
    return (before_ref[...].astype(F32) + linear * jax.nn.sigmoid(gate)).astype(BF16)


def update_kernel(own_ref, arrived_ref, before_ref, out):
    out[...] = updated(own_ref, arrived_ref, before_ref)


def merge_kernel(own_ref, arrived_ref, out):
    rows = own_ref.shape[1]
    me = lax.axis_index("dp")
    half = out.shape[2]
    out[:, pl.ds(pl.multiple_of(me * rows, rows), rows), :] = own_ref[:, :, :half]
    out[:, pl.ds(pl.multiple_of((1 - me) * rows, rows), rows), :] = arrived_ref[...]


def settle_kernel(chunk, *refs):
    pieces, out, sem = refs[:4], refs[4], refs[5]
    copies = []
    for i, (at, _) in enumerate(placed_pieces(pieces, chunk)):
        source = pieces[i // 4].at[(i // 2) % 2, i % 2]
        copies.append(pltpu.make_async_copy(source, out.at[:, pl.ds(at, chunk)], sem.at[i]))
        copies[-1].start()
    for copy in copies:
        copy.wait()


def settle(pieces, feats):
    rows, chunk = pieces[0].shape[2:]
    return pl.pallas_call(
        functools.partial(settle_kernel, chunk),
        in_specs=[VMEM] * 4,
        out_specs=ANY,
        out_shape=struct((rows, feats), BF16),
        scratch_shapes=[pltpu.SemaphoreType.DMA((16,))],
        compiler_params=params(4),
        name="settle",
    )(*pieces)


def plain_prepare(lengths, log_step, eig_re, eig_im, in_mat, output_matrices):
    factor = position_factor(lengths)
    step_size = jnp.exp(log_step)[:, None, :, None] * factor[None, :, None, None]
    eig_re, eig_im = eig_re[:, None], eig_im[:, None]
    magnitude = jnp.exp(eig_re * step_size)
    turned = eig_im * step_size
    decay_re = magnitude * jnp.cos(turned)
    decay_im = magnitude * jnp.sin(turned)
    modulus = eig_re * eig_re + eig_im * eig_im
    weight_re = ((decay_re - 1.0) * eig_re + decay_im * eig_im) / modulus
    weight_im = (decay_im * eig_re - (decay_re - 1.0) * eig_im) / modulus
    return jnp.stack([decay_re, decay_im, weight_re, weight_im], axis=1), in_mat, output_matrices


def plain_order(pieces, inner, outer):
    low, high = digits(inner)
    rows = []
    for h in range(outer):
        for l in range(inner):
            row = jnp.stack(pieces)[low ^ l, high ^ h]
            rows.append(row)
    return jnp.stack(rows)


def plain_recur(layer, dims, pieces, gains, weights, coeff, m, n, skip, state, so_far):
    dp, inner, outer, model, own, feats = dims
    groups, states = coeff.shape[3:]
    if layer > 0:
        rows = plain_order(pieces, inner, outer)
        rows = rows.reshape(inner * outer, own, dp, feats // (inner * outer))
        pieces = [rows[:, :, p].transpose(1, 0, 2).reshape(own, feats) for p in range(dp)]
    else:
        start = lax.axis_index("dp") * own
        pieces = [lax.dynamic_slice_in_dim(p, start, own, axis=0) for p in pieces]
    squares, partial_value = 0.0, 0.0
    for p in range(dp):
        current = pieces[p].astype(F32)
        squares = squares + jnp.sum(current * current, axis=1, keepdims=True)
        scaled = (current * gains[p][layer]).astype(BF16)
        partial_value = partial_value + jnp.dot(
            scaled, weights[p][layer], preferred_element_type=F32
        )
    driven = (partial_value * lax.rsqrt(squares / model + NORM_EPS)).astype(BF16).astype(F32)
    driven = driven.reshape(own, groups, -1)
    exact = lax.Precision.HIGHEST
    drive_re = jnp.einsum("bgc,gpc->bgp", driven, m[layer, 0], precision=exact)
    drive_im = jnp.einsum("bgc,gpc->bgp", driven, m[layer, 1], precision=exact)
    decay_re, decay_im, weight_re, weight_im = [coeff[layer, c] for c in range(4)]
    old_re, old_im = [state[layer, c].reshape(own, groups, states) for c in range(2)]
    new_re = decay_re * old_re - decay_im * old_im + weight_re * drive_re - weight_im * drive_im
    new_im = decay_re * old_im + decay_im * old_re + weight_re * drive_im + weight_im * drive_re
    value = jnp.einsum("bgp,gcp->bgc", new_re, n[layer, 0], precision=exact)
    value = value - jnp.einsum("bgp,gcp->bgc", new_im, n[layer, 1], precision=exact)
    value = value + skip[layer].reshape(groups, -1) * driven
    readout = jax.nn.gelu(value).reshape(own, -1).astype(BF16)
    new = jnp.stack([new_re, new_im]).reshape(1, 2, own, groups * states)
    if layer > 0:
        return readout, jnp.concatenate([so_far, new])
    chunk = feats // (inner * outer)
    start = lax.axis_index("tp") * chunk
    cuts = [lax.dynamic_slice_in_dim(p, start, chunk, axis=1) for p in pieces]
    return readout, new, jnp.concatenate(cuts, axis=1)


def plain_products(layer, dims, readout, weights):
    _, inner, outer, _, own, _ = dims
    terms = []
    for w in weights:
        term = jnp.dot(readout, w[layer], preferred_element_type=F32)
        terms.append(term.reshape(own, outer, inner, -1))
    terms = jnp.concatenate(terms, axis=3).transpose(2, 1, 0, 3)
    low, _ = digits(inner)
    outs = [terms[low ^ k] for k in range(inner)]
    return [outs[0]] + [o.astype(BF16) for o in outs[1:]]


def plain_fold(value, arrived):
    for a in arrived:
        value = value + a.astype(F32)
    _, high = digits(len(arrived) + 1)
    outs = [value[high ^ k] for k in range(value.shape[0])]
    return [outs[0]] + [o.astype(BF16) for o in outs[1:]]


def plain_update(block, arrived, before):
    for a in arrived:
        block = block + a.astype(F32)
    half = block.shape[1] // 2
    gated = block[:, :half] * jax.nn.sigmoid(block[:, half:])
    return (before.astype(F32) + gated).astype(BF16)


def plain_settle(pieces, feats):
    rows = plain_order(pieces, len(pieces), pieces[0].shape[0])
    return rows.transpose(1, 0, 2).reshape(rows.shape[1], feats)


def plain_layers(dims, layers, pieces, slabs_of, pointwise):
    dp, inner, outer, _, own, feats = dims
    gain_slabs, in_slabs, out_slabs = slabs_of
    lengths, log_step, eig_re, eig_im, in_mat, output_matrices, skip, state = pointwise
    tp = inner * outer
    chunk = feats // tp

    def over_low(value, k):
        return exchange(value, "tp", tp, 1, inner, k)

    def over_high(value, k):
        return exchange(value, "tp", tp, inner, outer, k)

    coeff, m, n = plain_prepare(lengths, log_step, eig_re, eig_im, in_mat, output_matrices)
    new_state = None
    for layer in range(layers):
        made = plain_recur(
            layer, dims, pieces, gain_slabs, in_slabs, coeff, m, n, skip, state, new_state
        )
        readout, new_state = made[:2]
        if layer == 0:
            before = made[2]
        sends = plain_products(layer, dims, readout, out_slabs)
        arrived = [over_low(sends[k], k) for k in range(1, inner)]
        sends = plain_fold(sends[0], arrived)
        arrived = [over_high(sends[k], k) for k in range(1, outer)]
        shard = plain_update(sends[0], arrived, before)
        before = shard
        if layer + 1 == layers:
            cuts = [shard[:, k * chunk : (k + 1) * chunk] for k in range(dp)]
            here = [cuts[0]] + [exchange(cuts[k], "dp", dp, 1, dp, k) for k in range(1, dp)]
            order = lax.axis_index("dp") ^ jnp.arange(dp)
            shard = jnp.stack(here)[order].reshape(own * dp, chunk)
        column = jnp.stack([shard] + [over_high(shard, k) for k in range(1, outer)])
        pieces = [column] + [over_low(column, k) for k in range(1, inner)]
    return plain_settle(pieces, feats), new_state


def kernel_layers(dims, tokens, norm_gain, w_in, w_glu, w_gate, pointwise):
    dp, _, _, _, own, feats = dims
    lengths, log_step, eig_re, eig_im, in_mat, output_matrices, skip, state = pointwise
    layers = w_in.shape[0]
    chunk = feats // 16
    wide = 2 * dp * chunk

    def core_swap(value):
        return exchange(value, "dp", 2, 1, 2, 1)

    def over_low(value, k):
        return exchange(value, "tp", 16, 1, 4, k)

    def over_near(value):
        return exchange(value, "tp", 16, 4, 2, 1)

    def over_far(value):
        return exchange(value, "tp", 16, 8, 2, 1)

    width = skip.shape[1]
    others = (
        lengths[None, :],
        log_step,
        eig_re,
        eig_im,
        jnp.swapaxes(in_mat, 3, 4).reshape(layers, 2, width, -1),
        output_matrices.reshape(layers, 2, width, -1),
        skip,
        state,
    )
    keep, send, others, outward = project(
        dims, tokens, norm_gain, w_in, others, (w_glu, w_gate)
    )
    pieces = [keep, core_swap(send)]
    outward = [outward[0], core_swap(outward[0]), outward[1], core_swap(outward[1])]
    consts = (*prepare(own, *others[:6]), *others[6:])

    readout, new_state, before = recur(0, dims, consts, pieces, [], None)
    parts = products(dims, readout, outward)
    arrived = [over_low(parts[k], k) for k in range(1, 4)]
    stacks = lax.optimization_barrier((w_in, w_glu, w_gate, norm_gain, parts[0]))
    inward, *packs = pack(*stacks[:3])
    gain = stacks[3]
    slabs = [norm_gain, core_swap(gain), inward, core_swap(inward)]
    keep, send = call(
        fold_low_kernel,
        (parts[0], *arrived),
        [struct((2, own, wide), F32), struct((2, own, wide), BF16)],
    )
    arrived = over_near(send)
    *packs, _ = lax.optimization_barrier((*packs, send))
    weights = [packs[0]] + [over_low(packs[k], k) for k in range(1, 4)]
    (send,) = call(fold_near_kernel, (keep, arrived), [struct((2, own, wide), BF16)])
    terms = (send, over_far(send), before)
    (shard,) = call(update_kernel, terms, [struct((2, own, dp * chunk), BF16)])
    column = jnp.stack([shard, over_near(shard)])
    pieces = [column] + [over_low(column, k) for k in range(1, 4)]
    away, _ = lax.optimization_barrier((shard[:, :, chunk:], column))
    away = core_swap(away)
    (before,) = call(merge_kernel, (shard, away), [struct((2, own * dp, chunk), BF16)])

    readout, new_state = recur(1, dims, consts, pieces, slabs, new_state)
    readout = readout[None]
    (rows,) = call(
        merge_kernel, (readout, core_swap(readout)), [struct((1, own * dp, width), BF16)]
    )
    rows = rows[0]
    readouts = [rows] + [over_low(rows, k) for k in range(1, 4)]
    keep, send = gathered_products(chunk, readouts, weights)
    (send,) = call(
        fold_near_kernel, (keep, over_near(send)), [struct((2, own * dp, 2 * chunk), BF16)]
    )
    terms = (send, over_far(send), before)
    (shard,) = call(update_kernel, terms, [struct((2, own * dp, chunk), BF16)])
    column = jnp.stack([shard, over_near(shard)])
    pieces = [column] + [over_low(column, k) for k in range(1, 4)]
    return settle(pieces, feats), new_state


def make_body(tp, dp):
    inner = 1 << (int(math.log2(tp)) // 2)
    outer = tp // inner

    def body(
        tokens,
        lengths,
        norm_gain,
        w_in,
        log_step,
        eig_re,
        eig_im,
        in_mat,
        output_matrices,
        skip,
        w_glu,
        w_gate,
        state,
    ):
        layers = w_in.shape[0]
        seqs, feats = tokens.shape
        own = seqs // dp
        chunk = feats // tp
        dims = (dp, inner, outer, feats * dp, own, feats)
        pointwise = (lengths, log_step, eig_re, eig_im, in_mat, output_matrices, skip, state)
        regular = tp == 16 and dp == 2 and layers == 2 and chunk % 128 == 0 and own % 16 == 0
        if regular and skip.shape[1] % 128 == 0:
            return kernel_layers(dims, tokens, norm_gain, w_in, w_glu, w_gate, pointwise)

        def slabs(value):
            return [value] + [exchange(value, "dp", dp, 1, dp, k) for k in range(1, dp)]

        slabs_of = (slabs(norm_gain), slabs(w_in), slabs(w_glu) + slabs(w_gate))
        return plain_layers(dims, layers, slabs(tokens), slabs_of, pointwise)

    return body


def solution(mesh):
    placed = (
        P(None, "dp"),
        P("dp"),
        P(None, "dp"),
        P(None, "dp", "tp"),
        P(None, "tp"),
        P(None, "tp", None),
        P(None, "tp", None),
        P(None, None, "tp", None, None),
        P(None, None, "tp", None, None),
        P(None, "tp"),
        P(None, "tp", "dp"),
        P(None, "tp", "dp"),
        P(None, None, "dp", "tp"),
    )
    return jax.shard_map(
        make_body(mesh.shape["tp"], mesh.shape["dp"]),
        mesh=mesh,
        in_specs=placed,
        out_specs=(P(None, "dp"), P(None, None, "dp", "tp")),
        check_vma=False,
    )
```

```python
import functools
import math

import jax
import jax.numpy as jnp
from jax import lax
from jax.experimental import pallas as pl
from jax.experimental.pallas import tpu as pltpu
from jax.sharding import PartitionSpec as P


BLOCK_LEN = 256
LEN_MAX = 4096
NORM_EPS = 1e-06
F32 = jnp.float32
BF16 = jnp.bfloat16


def position_factor(lengths):
    blocks = (lengths // BLOCK_LEN).astype(F32)
    return 2.0 / (1.0 + blocks * (4.0 * BLOCK_LEN / LEN_MAX))


def exchange(value, axis, size, stride, count, k):
    pairs = []
    for i in range(size):
        digit = (i // stride) % count
        pairs.append((i, i + ((digit ^ k) - digit) * stride))
    return lax.ppermute(value, axis, pairs)


def params(mib=16):
    return pltpu.CompilerParams(vmem_limit_bytes=mib << 20)


VMEM = pl.BlockSpec(memory_space=pltpu.VMEM)
ANY = pl.BlockSpec(memory_space=pl.ANY)
HBM = pl.BlockSpec(memory_space=pltpu.HBM)


def struct(shape, dtype):
    return jax.ShapeDtypeStruct(shape, dtype)


def nt_dot(a, b):
    return lax.dot_general(a, b, (((1,), (1,)), ((), ())), preferred_element_type=F32)


def digits(inner):
    index = lax.axis_index("tp")
    return index % inner, index // inner


def call(kernel, args, outs, scratch=(), mib=4):
    return pl.pallas_call(
        kernel,
        in_specs=[VMEM] * len(args),
        out_specs=[VMEM] * len(outs),
        out_shape=outs,
        scratch_shapes=scratch,
        compiler_params=params(mib),
        cost_estimate=pl.CostEstimate(flops=1 << 22, bytes_accessed=1 << 20, transcendentals=0),
    )(*args)


def corner():
    index = lax.axis_index("tp")
    return index % 4, (index // 4) % 2, index // 8


def placed_sources(pieces, chunk):
    low, near, _ = corner()
    for k, piece in enumerate(pieces):
        if piece is not None:
            for j in range(2):
                for far in range(2):
                    at = ((2 * far + (near ^ j)) * 4 + (low ^ k)) * chunk
                    yield pl.multiple_of(at, chunk), k, piece.at[j, far]


def iota(shape, axis):
    return lax.broadcasted_iota(jnp.int32, shape, axis)


def exact_dot(a, b):
    return jnp.dot(a, b, precision=lax.Precision.HIGHEST, preferred_element_type=F32)


def prepare_kernel(
    layer, lengths_ref, step_ref, re_ref, im_ref, in_ref, out_ref, coeff_ref, m_ref, n_ref
):
    _, groups, states = re_ref.shape
    total, width = coeff_ref.shape[2], n_ref.shape[1]
    group = width // groups
    own = lengths_ref.shape[1]
    row = jnp.broadcast_to(position_factor(lengths_ref[...]), (own, own))
    factor = jnp.sum(
        jnp.where(iota((own, own), 0) == iota((own, own), 1), row, 0.0), axis=1, keepdims=True
    )
    spread = (iota((states, total), 1) % states == iota((states, total), 0)).astype(F32)
    spread_half = spread.astype(BF16)
    of_group = iota((groups, total), 1) // states == iota((groups, total), 0)
    keep = iota((width, total), 0) // group == iota((width, total), 1) // states

    def flat(value):
        return jnp.sum(
            jnp.where(of_group, exact_dot(value, spread), 0.0), axis=0, keepdims=True
        )

    log_step = exact_dot(step_ref[layer : layer + 1, :], of_group.astype(F32))
    eig_re = flat(re_ref[layer])
    eig_im = flat(im_ref[layer])
    step_size = jnp.exp(log_step) * factor
    magnitude = jnp.exp(eig_re * step_size)
    turned = eig_im * step_size
    decay_re = magnitude * jnp.cos(turned)
    decay_im = magnitude * jnp.sin(turned)
    scale = 1.0 / (eig_re * eig_re + eig_im * eig_im)
    coeff_ref[0] = decay_re
    coeff_ref[1] = decay_im
    coeff_ref[2] = ((decay_re - 1.0) * eig_re + decay_im * eig_im) * scale
    coeff_ref[3] = (decay_im * eig_re - (decay_re - 1.0) * eig_im) * scale
    for part in range(2):
        for source, target in ((in_ref, m_ref), (out_ref, n_ref)):
            value = jnp.dot(
                source[layer, part].astype(BF16), spread_half, preferred_element_type=F32
            )
            if part == 1 and target is n_ref:
                value = -value
            target[part] = jnp.where(keep, value, 0.0).astype(BF16)


def prepare(layer, own, lengths, log_step, eig_re, eig_im, in_rows, out_rows):
    _, groups, states = eig_re.shape
    total, width = groups * states, in_rows.shape[2]
    outs = [
        struct((4, own, total), F32),
        struct((2, width, total), BF16),
        struct((2, width, total), BF16),
    ]
    args = (lengths, log_step, eig_re, eig_im, in_rows, out_rows)
    return call(functools.partial(prepare_kernel, layer), args, outs)


def pack_kernel(in_hbm, glu_hbm, gate_hbm, in_out, *refs):
    packs, sem, sems = refs[:4], refs[4], refs[5]
    chunk = packs[0].shape[1] // 8
    low, _, _ = corner()
    copies = [pltpu.make_async_copy(in_hbm.at[1], in_out, sem)]
    for k in range(4):
        for w, source in enumerate((glu_hbm, gate_hbm)):
            for h in range(4):
                at = pl.multiple_of((h * 4 + (low ^ k)) * chunk, chunk)
                copies.append(
                    pltpu.make_async_copy(
                        source.at[1, :, pl.ds(at, chunk)],
                        packs[k].at[:, (w * 4 + h) * chunk : (w * 4 + h + 1) * chunk],
                        sems.at[k, w, h],
                    )
                )
    for copy in copies:
        copy.start()
    for copy in copies:
        copy.wait()


def pack(w_in, w_glu, w_gate):
    width, chunk = w_glu.shape[1], w_glu.shape[2] // 16
    args = [pltpu.with_memory_space_constraint(a, pltpu.HBM) for a in (w_in, w_glu, w_gate)]
    outs = [pltpu.VMEM(w_in.shape[1:], BF16)] + [pltpu.VMEM((width, 8 * chunk), BF16)] * 4
    return pl.pallas_call(
        pack_kernel,
        in_specs=[HBM] * 3,
        out_specs=[VMEM] * 5,
        out_shape=outs,
        scratch_shapes=[pltpu.SemaphoreType.DMA, pltpu.SemaphoreType.DMA((4, 2, 4))],
        compiler_params=params(4),
        cost_estimate=pl.CostEstimate(flops=8 << 20, bytes_accessed=3 << 20, transcendentals=0),
        name="pack",
    )(*args)


def project_kernel(count, *refs):
    tokens_hbm, gain_hbm, weight_hbm = refs[:3]
    sources, (keep, send), targets = refs[3 : 3 + count], refs[3 + count : 5 + count], refs[5 + count : -4]
    tokens, gain, weight, sems = refs[-4:]
    pairs = [(tokens_hbm, tokens), (gain_hbm, gain), (weight_hbm.at[0], weight)]
    pairs += [(a.at[0] if len(a.shape) > len(b.shape) else a, b) for a, b in zip(sources, targets)]
    copies = [pltpu.make_async_copy(a, b, sems.at[i]) for i, (a, b) in enumerate(pairs)]
    for copy in copies:
        copy.start()
    own, width = keep.shape[0], weight.shape[1]
    chunk = tokens.shape[1] // 16
    copies[0].wait()
    copies[1].wait()
    current = tokens[...].astype(F32)
    squares = jnp.sum(current * current, axis=1, keepdims=True)
    scaled = (current * gain[0:1, :]).astype(BF16)
    copies[2].wait()
    term = jnp.dot(scaled, weight[...], preferred_element_type=F32)
    low, near, _ = corner()
    me = lax.axis_index("dp")
    for out, flip in ((keep, me), (send, 1 - me)):
        upper = flip == 1
        out[:, :width] = jnp.where(upper, term[own:], term[:own])
        out[:, width : width + 128] = jnp.broadcast_to(
            jnp.where(upper, squares[own:], squares[:own]), (own, 128)
        )
        start = pl.multiple_of(flip * own, own)
        for far in range(2):
            at = pl.multiple_of(((2 * far + near) * 4 + low) * chunk, chunk)
            base = width + 128 + far * chunk
            out[:, base : base + chunk] = tokens[pl.ds(start, own), pl.ds(at, chunk)].astype(F32)
    for copy in copies[3:]:
        copy.wait()


def project(dims, tokens, gain, weight, others, stacks):
    _, _, _, _, own, feats = dims
    width = weight.shape[2]
    shape = (own, width + 128 + 2 * feats // 16)
    args = [pltpu.with_memory_space_constraint(a, pltpu.HBM) for a in (tokens, gain, weight, *others, *stacks)]
    made = pl.pallas_call(
        functools.partial(project_kernel, len(others) + len(stacks)),
        in_specs=[HBM] * len(args),
        out_specs=[VMEM] * (2 + len(others) + len(stacks)),
        out_shape=[struct(shape, F32)] * 2 + [pltpu.VMEM(a.shape, a.dtype) for a in others]
        + [pltpu.VMEM(a.shape[1:], a.dtype) for a in stacks],
        scratch_shapes=[
            pltpu.VMEM(tokens.shape, BF16),
            pltpu.VMEM(gain.shape, F32),
            pltpu.VMEM(weight.shape[1:], BF16),
            pltpu.SemaphoreType.DMA((len(args),)),
        ],
        compiler_params=params(4),
        cost_estimate=pl.CostEstimate(flops=32 << 20, bytes_accessed=1 << 20, transcendentals=0),
        name="project",
    )(*args)
    return made[0], made[1], made[2 : 2 + len(others)], made[2 + len(others) :]


def piece_kernel(k, dp, layer, piece, *refs):
    gains, weights, (partial_out, squares_out) = refs[:dp], refs[dp : 2 * dp], refs[2 * dp :]
    own, chunk = piece.shape[2], piece.shape[3] // dp
    low, near, _ = corner()
    squares = jnp.zeros((own, 1), F32)
    partial_value = jnp.zeros(partial_out.shape, F32)
    for j in range(2):
        for far in range(2):
            at = ((2 * far + (near ^ j)) * 4 + (low ^ k)) * chunk
            at = pl.multiple_of(at, chunk)
            for p in range(dp):
                current = piece[j, far, :, p * chunk : (p + 1) * chunk].astype(F32)
                squares = squares + jnp.sum(current * current, axis=1, keepdims=True)
                gain = gains[p][layer : layer + 1, pl.ds(at, chunk)]
                scaled = (current * gain).astype(BF16)
                partial_value = partial_value + jnp.dot(
                    scaled, weights[p][pl.ds(at, chunk), :], preferred_element_type=F32
                )
    partial_out[...] = partial_value
    squares_out[...] = jnp.broadcast_to(squares, squares_out.shape)


def project_piece(k, layer, piece, gains, weights):
    own = piece.shape[2]
    dp = len(gains)
    width = weights[0].shape[1]
    return call(
        functools.partial(piece_kernel, k, dp, layer),
        (piece, *gains, *weights),
        [struct((own, width), F32), struct((own, 128), F32)],
    )


def recur_kernel(layer, dp, model, *refs):
    coeff_ref, m_ref, n_ref, skip_ref, state_ref = refs[:5]
    width = skip_ref.shape[1]
    if layer == 0:
        pieces, (readout_ref, new_ref, before_ref) = refs[5:7], refs[7:]
        chunk = before_ref.shape[2] // dp
        partial_value = pieces[0][:, :width] + pieces[1][:, :width]
        squares = (pieces[0][:, width : width + 128] + pieces[1][:, width : width + 128])[:, :1]
        for far in range(2):
            for p in range(dp):
                base = width + 128 + far * chunk
                before_ref[far, :, p * chunk : (p + 1) * chunk] = pieces[p][
                    :, base : base + chunk
                ].astype(BF16)
    else:
        terms, (readout_ref, new_ref) = refs[5:13], refs[13:]
        partial_value = terms[0][...] + terms[2][...] + terms[4][...] + terms[6][...]
        squares = terms[1][...] + terms[3][...] + terms[5][...] + terms[7][...]
        squares = squares[:, :1]
    driven = (partial_value * lax.rsqrt(squares / model + NORM_EPS)).astype(BF16)
    drive_re = jnp.dot(driven, m_ref[0], preferred_element_type=F32)
    drive_im = jnp.dot(driven, m_ref[1], preferred_element_type=F32)
    decay_re, decay_im = coeff_ref[0], coeff_ref[1]
    weight_re, weight_im = coeff_ref[2], coeff_ref[3]
    old_re, old_im = state_ref[layer, 0], state_ref[layer, 1]
    new_re = decay_re * old_re - decay_im * old_im + weight_re * drive_re - weight_im * drive_im
    new_im = decay_re * old_im + decay_im * old_re + weight_re * drive_im + weight_im * drive_re
    new_ref[0] = new_re
    new_ref[1] = new_im
    value = nt_dot(new_re.astype(BF16), n_ref[0])
    value = value + nt_dot(new_im.astype(BF16), n_ref[1])
    value = value + skip_ref[layer : layer + 1, :] * driven.astype(F32)
    readout_ref[...] = jax.nn.gelu(value).astype(BF16)


def recur(layer, dims, consts, terms):
    dp, _, _, model, own, feats = dims
    skip, state = consts[3:]
    outs = [struct((own, skip.shape[1]), BF16), pltpu.VMEM(state.shape[1:], F32)]
    if layer == 0:
        outs.append(struct((2, own, dp * feats // 16), BF16))
    return call(functools.partial(recur_kernel, layer, dp, model), (*consts, *terms), outs, mib=8)


def store_kernel(first, second, out, sems):
    copies = [
        pltpu.make_async_copy(ref, out.at[layer], sems.at[layer])
        for layer, ref in enumerate((first, second))
    ]
    for copy in copies:
        copy.start()
    for copy in copies:
        copy.wait()


def store(states):
    return pl.pallas_call(
        store_kernel,
        in_specs=[VMEM] * 2,
        out_specs=ANY,
        out_shape=struct((2,) + states[0].shape, F32),
        scratch_shapes=[pltpu.SemaphoreType.DMA((2,))],
        compiler_params=params(4),
        cost_estimate=pl.CostEstimate(flops=1 << 20, bytes_accessed=1 << 19, transcendentals=0),
        name="store",
    )(*states)


def product_kernel(chunk, readout_ref, *refs):
    weights, outs, spread = refs[:-5], refs[-5:-1], refs[-1]
    count = len(weights)
    low, _, _ = corner()
    readout = readout_ref[...]
    for w in range(count):
        value = jnp.dot(readout, weights[w][...], preferred_element_type=F32)
        for j in range(16):
            spread[w, j] = value[:, j * chunk : (j + 1) * chunk]
    for k in range(4):
        for h in range(4):
            for w in range(count):
                outs[k][h, :, w * chunk : (w + 1) * chunk] = spread[w, h * 4 + (low ^ k)].astype(
                    outs[k].dtype
                )


def products(dims, readout, weights):
    _, _, _, _, own, feats = dims
    chunk = feats // 16
    shape = (4, own, len(weights) * chunk)
    return call(
        functools.partial(product_kernel, chunk),
        (readout, *weights),
        [struct(shape, F32)] + [struct(shape, BF16)] * 3,
        [pltpu.VMEM((len(weights), 16, own, chunk), F32)],
        8,
    )


def gathered_kernel(chunk, *refs):
    readouts, weights, (keep, send, spread) = refs[:4], refs[4:8], refs[8:]
    _, near, _ = corner()
    value = None
    for k in range(4):
        term = jnp.dot(readouts[k][...], weights[k][...], preferred_element_type=F32)
        value = term if value is None else value + term
    for j in range(8):
        spread[j] = value[:, j * chunk : (j + 1) * chunk]
    for far in range(2):
        for w in range(2):
            lanes = slice(w * chunk, (w + 1) * chunk)
            at = w * 4 + 2 * far + near
            keep[far, :, lanes] = spread[at]
            send[far, :, lanes] = spread[w * 4 + 2 * far + (near ^ 1)].astype(BF16)


def gathered_products(chunk, readouts, weights):
    rows = readouts[0].shape[0]
    return call(
        functools.partial(gathered_kernel, chunk),
        (*readouts, *weights),
        [struct((2, rows, 2 * chunk), F32), struct((2, rows, 2 * chunk), BF16)],
        [pltpu.VMEM((8, rows, chunk), F32)],
        8,
    )


def fold_low_kernel(own_ref, a_ref, b_ref, c_ref, keep, send):
    _, near, _ = corner()
    for far in range(2):
        for out, turn in ((keep, 0), (send, 1)):
            at = 2 * far + (near ^ turn)
            total = own_ref[at] + a_ref[at].astype(F32) + b_ref[at].astype(F32)
            out[far] = (total + c_ref[at].astype(F32)).astype(out.dtype)


def fold_near_kernel(own_ref, arrived_ref, send):
    send[...] = (own_ref[...] + arrived_ref[...].astype(F32)).astype(BF16)


def updated(own_ref, arrived_ref, before_ref):
    total = own_ref[...].astype(F32) + arrived_ref[...].astype(F32)
    half = total.shape[2] // 2
    linear, gate = total[:, :, :half], total[:, :, half:]
    return (before_ref[...].astype(F32) + linear * jax.nn.sigmoid(gate)).astype(BF16)


def update_kernel(own_ref, arrived_ref, before_ref, out):
    out[...] = updated(own_ref, arrived_ref, before_ref)


def merge_kernel(own_ref, arrived_ref, out):
    rows = own_ref.shape[1]
    me = lax.axis_index("dp")
    half = out.shape[2]
    out[:, pl.ds(pl.multiple_of(me * rows, rows), rows), :] = own_ref[:, :, :half]
    out[:, pl.ds(pl.multiple_of((1 - me) * rows, rows), rows), :] = arrived_ref[...]


def settle_kernel(which, chunk, *refs):
    pieces, out, sem = refs[: len(which)], refs[-2], refs[-1]
    slots = [None] * 4
    for k, piece in zip(which, pieces):
        slots[k] = piece
    copies = []
    for at, k, source in placed_sources(slots, chunk):
        copies.append(
            pltpu.make_async_copy(source, out.at[:, pl.ds(at, chunk)], sem.at[len(copies)])
        )
        copies[-1].start()
    for copy in copies:
        copy.wait()


def settle(which, pieces, feats, so_far=None):
    rows, chunk = pieces[0].shape[2:]
    args = [pieces[k] for k in which]
    specs = [VMEM] * len(args)
    alias = {}
    if so_far is not None:
        alias = {len(args): 0}
        args.append(so_far)
        specs.append(ANY)
    return pl.pallas_call(
        functools.partial(settle_kernel, which, chunk),
        in_specs=specs,
        out_specs=ANY,
        out_shape=struct((rows, feats), BF16),
        scratch_shapes=[pltpu.SemaphoreType.DMA((4 * len(which),))],
        input_output_aliases=alias,
        compiler_params=params(4),
        cost_estimate=pl.CostEstimate(flops=1 << 20, bytes_accessed=1 << 18, transcendentals=0),
        name="settle",
    )(*args)


def plain_prepare(lengths, log_step, eig_re, eig_im, in_mat, output_matrices):
    factor = position_factor(lengths)
    step_size = jnp.exp(log_step)[:, None, :, None] * factor[None, :, None, None]
    eig_re, eig_im = eig_re[:, None], eig_im[:, None]
    magnitude = jnp.exp(eig_re * step_size)
    turned = eig_im * step_size
    decay_re = magnitude * jnp.cos(turned)
    decay_im = magnitude * jnp.sin(turned)
    modulus = eig_re * eig_re + eig_im * eig_im
    weight_re = ((decay_re - 1.0) * eig_re + decay_im * eig_im) / modulus
    weight_im = (decay_im * eig_re - (decay_re - 1.0) * eig_im) / modulus
    return jnp.stack([decay_re, decay_im, weight_re, weight_im], axis=1), in_mat, output_matrices


def plain_order(pieces, inner, outer):
    low, high = digits(inner)
    rows = []
    for h in range(outer):
        for l in range(inner):
            row = jnp.stack(pieces)[low ^ l, high ^ h]
            rows.append(row)
    return jnp.stack(rows)


def plain_recur(layer, dims, pieces, gains, weights, coeff, m, n, skip, state, so_far):
    dp, inner, outer, model, own, feats = dims
    groups, states = coeff.shape[3:]
    if layer > 0:
        rows = plain_order(pieces, inner, outer)
        rows = rows.reshape(inner * outer, own, dp, feats // (inner * outer))
        pieces = [rows[:, :, p].transpose(1, 0, 2).reshape(own, feats) for p in range(dp)]
    else:
        start = lax.axis_index("dp") * own
        pieces = [lax.dynamic_slice_in_dim(p, start, own, axis=0) for p in pieces]
    squares, partial_value = 0.0, 0.0
    for p in range(dp):
        current = pieces[p].astype(F32)
        squares = squares + jnp.sum(current * current, axis=1, keepdims=True)
        scaled = (current * gains[p][layer]).astype(BF16)
        partial_value = partial_value + jnp.dot(
            scaled, weights[p][layer], preferred_element_type=F32
        )
    driven = (partial_value * lax.rsqrt(squares / model + NORM_EPS)).astype(BF16).astype(F32)
    driven = driven.reshape(own, groups, -1)
    exact = lax.Precision.HIGHEST
    drive_re = jnp.einsum("bgc,gpc->bgp", driven, m[layer, 0], precision=exact)
    drive_im = jnp.einsum("bgc,gpc->bgp", driven, m[layer, 1], precision=exact)
    decay_re, decay_im, weight_re, weight_im = [coeff[layer, c] for c in range(4)]
    old_re, old_im = [state[layer, c].reshape(own, groups, states) for c in range(2)]
    new_re = decay_re * old_re - decay_im * old_im + weight_re * drive_re - weight_im * drive_im
    new_im = decay_re * old_im + decay_im * old_re + weight_re * drive_im + weight_im * drive_re
    value = jnp.einsum("bgp,gcp->bgc", new_re, n[layer, 0], precision=exact)
    value = value - jnp.einsum("bgp,gcp->bgc", new_im, n[layer, 1], precision=exact)
    value = value + skip[layer].reshape(groups, -1) * driven
    readout = jax.nn.gelu(value).reshape(own, -1).astype(BF16)
    new = jnp.stack([new_re, new_im]).reshape(1, 2, own, groups * states)
    if layer > 0:
        return readout, jnp.concatenate([so_far, new])
    chunk = feats // (inner * outer)
    start = lax.axis_index("tp") * chunk
    cuts = [lax.dynamic_slice_in_dim(p, start, chunk, axis=1) for p in pieces]
    return readout, new, jnp.concatenate(cuts, axis=1)


def plain_products(layer, dims, readout, weights):
    _, inner, outer, _, own, _ = dims
    terms = []
    for w in weights:
        term = jnp.dot(readout, w[layer], preferred_element_type=F32)
        terms.append(term.reshape(own, outer, inner, -1))
    terms = jnp.concatenate(terms, axis=3).transpose(2, 1, 0, 3)
    low, _ = digits(inner)
    outs = [terms[low ^ k] for k in range(inner)]
    return [outs[0]] + [o.astype(BF16) for o in outs[1:]]


def plain_fold(value, arrived):
    for a in arrived:
        value = value + a.astype(F32)
    _, high = digits(len(arrived) + 1)
    outs = [value[high ^ k] for k in range(value.shape[0])]
    return [outs[0]] + [o.astype(BF16) for o in outs[1:]]


def plain_update(block, arrived, before):
    for a in arrived:
        block = block + a.astype(F32)
    half = block.shape[1] // 2
    gated = block[:, :half] * jax.nn.sigmoid(block[:, half:])
    return (before.astype(F32) + gated).astype(BF16)


def plain_settle(pieces, feats):
    rows = plain_order(pieces, len(pieces), pieces[0].shape[0])
    return rows.transpose(1, 0, 2).reshape(rows.shape[1], feats)


def plain_layers(dims, layers, pieces, slabs_of, pointwise):
    dp, inner, outer, _, own, feats = dims
    gain_slabs, in_slabs, out_slabs = slabs_of
    lengths, log_step, eig_re, eig_im, in_mat, output_matrices, skip, state = pointwise
    tp = inner * outer
    chunk = feats // tp

    def over_low(value, k):
        return exchange(value, "tp", tp, 1, inner, k)

    def over_high(value, k):
        return exchange(value, "tp", tp, inner, outer, k)

    coeff, m, n = plain_prepare(lengths, log_step, eig_re, eig_im, in_mat, output_matrices)
    new_state = None
    for layer in range(layers):
        made = plain_recur(
            layer, dims, pieces, gain_slabs, in_slabs, coeff, m, n, skip, state, new_state
        )
        readout, new_state = made[:2]
        if layer == 0:
            before = made[2]
        sends = plain_products(layer, dims, readout, out_slabs)
        arrived = [over_low(sends[k], k) for k in range(1, inner)]
        sends = plain_fold(sends[0], arrived)
        arrived = [over_high(sends[k], k) for k in range(1, outer)]
        shard = plain_update(sends[0], arrived, before)
        before = shard
        if layer + 1 == layers:
            cuts = [shard[:, k * chunk : (k + 1) * chunk] for k in range(dp)]
            here = [cuts[0]] + [exchange(cuts[k], "dp", dp, 1, dp, k) for k in range(1, dp)]
            order = lax.axis_index("dp") ^ jnp.arange(dp)
            shard = jnp.stack(here)[order].reshape(own * dp, chunk)
        column = jnp.stack([shard] + [over_high(shard, k) for k in range(1, outer)])
        pieces = [column] + [over_low(column, k) for k in range(1, inner)]
    return plain_settle(pieces, feats), new_state


def kernel_layers(dims, tokens, norm_gain, w_in, w_glu, w_gate, pointwise):
    dp, _, _, _, own, feats = dims
    lengths, log_step, eig_re, eig_im, in_mat, output_matrices, skip, state = pointwise
    layers = w_in.shape[0]
    chunk = feats // 16
    wide = 2 * dp * chunk

    def core_swap(value):
        return exchange(value, "dp", 2, 1, 2, 1)

    def over_low(value, k):
        return exchange(value, "tp", 16, 1, 4, k)

    def over_near(value):
        return exchange(value, "tp", 16, 4, 2, 1)

    def over_far(value):
        return exchange(value, "tp", 16, 8, 2, 1)

    width = skip.shape[1]
    others = (
        lengths[None, :],
        log_step,
        eig_re,
        eig_im,
        jnp.swapaxes(in_mat, 3, 4).reshape(layers, 2, width, -1),
        output_matrices.reshape(layers, 2, width, -1),
        skip,
        state,
    )
    keep, send, others, outward = project(
        dims, tokens, norm_gain, w_in, others, (w_glu, w_gate)
    )
    pieces = [keep, core_swap(send)]
    outward = [outward[0], core_swap(outward[0]), outward[1], core_swap(outward[1])]
    consts = (*prepare(0, own, *others[:6]), *others[6:])

    readout, new_first, before = recur(0, dims, consts, pieces)
    parts = products(dims, readout, outward)
    arrived = [over_low(parts[k], k) for k in range(1, 4)]
    stacks = lax.optimization_barrier((w_in, w_glu, w_gate, norm_gain, parts[0]))
    inward, *packs = pack(*stacks[:3])
    gain = stacks[3]
    *others, _ = lax.optimization_barrier((*others, parts[0]))
    later_consts = (*prepare(1, own, *others[:6]), *others[6:])
    slabs = [norm_gain, core_swap(gain), inward, core_swap(inward)]
    keep, send = call(
        fold_low_kernel,
        (parts[0], *arrived),
        [struct((2, own, wide), F32), struct((2, own, wide), BF16)],
    )
    arrived = over_near(send)
    *packs, _ = lax.optimization_barrier((*packs, send))
    weights = [packs[0]] + [over_low(packs[k], k) for k in range(1, 4)]
    (send,) = call(fold_near_kernel, (keep, arrived), [struct((2, own, wide), BF16)])
    terms = (send, over_far(send), before)
    (shard,) = call(update_kernel, terms, [struct((2, own, dp * chunk), BF16)])
    column = jnp.stack([shard, over_near(shard)])
    pieces = [column] + [over_low(column, k) for k in range(1, 4)]
    away, _ = lax.optimization_barrier((shard[:, :, chunk:], column))
    away = core_swap(away)
    (before,) = call(merge_kernel, (shard, away), [struct((2, own * dp, chunk), BF16)])

    terms = []
    for k in (0, 3, 2, 1):
        terms += project_piece(k, 1, pieces[k], slabs[:2], slabs[2:])
    readout, new_second = recur(1, dims, later_consts, terms)
    readout = readout[None]
    (rows,) = call(
        merge_kernel, (readout, core_swap(readout)), [struct((1, own * dp, width), BF16)]
    )
    rows = rows[0]
    readouts = [rows] + [over_low(rows, k) for k in range(1, 4)]
    keep, send = gathered_products(chunk, readouts, weights)
    arrived = over_near(send)
    (send,) = call(fold_near_kernel, (keep, arrived), [struct((2, own * dp, 2 * chunk), BF16)])
    new_state = store([new_first, new_second])
    terms = (send, over_far(send), before)
    (shard,) = call(update_kernel, terms, [struct((2, own * dp, chunk), BF16)])
    column = jnp.stack([shard, over_near(shard)])
    pieces = [column] + [over_low(column, k) for k in range(1, 4)]
    mixed = settle((0, 3), pieces, feats)
    return settle((1, 2), pieces, feats, mixed), new_state


def make_body(tp, dp):
    inner = 1 << (int(math.log2(tp)) // 2)
    outer = tp // inner

    def body(
        tokens,
        lengths,
        norm_gain,
        w_in,
        log_step,
        eig_re,
        eig_im,
        in_mat,
        output_matrices,
        skip,
        w_glu,
        w_gate,
        state,
    ):
        layers = w_in.shape[0]
        seqs, feats = tokens.shape
        own = seqs // dp
        chunk = feats // tp
        dims = (dp, inner, outer, feats * dp, own, feats)
        pointwise = (lengths, log_step, eig_re, eig_im, in_mat, output_matrices, skip, state)
        regular = tp == 16 and dp == 2 and layers == 2 and chunk % 128 == 0 and own % 16 == 0
        if regular and skip.shape[1] % 128 == 0:
            return kernel_layers(dims, tokens, norm_gain, w_in, w_glu, w_gate, pointwise)

        def slabs(value):
            return [value] + [exchange(value, "dp", dp, 1, dp, k) for k in range(1, dp)]

        slabs_of = (slabs(norm_gain), slabs(w_in), slabs(w_glu) + slabs(w_gate))
        return plain_layers(dims, layers, slabs(tokens), slabs_of, pointwise)

    return body


def solution(mesh):
    placed = (
        P(None, "dp"),
        P("dp"),
        P(None, "dp"),
        P(None, "dp", "tp"),
        P(None, "tp"),
        P(None, "tp", None),
        P(None, "tp", None),
        P(None, None, "tp", None, None),
        P(None, None, "tp", None, None),
        P(None, "tp"),
        P(None, "tp", "dp"),
        P(None, "tp", "dp"),
        P(None, None, "dp", "tp"),
    )
    return jax.shard_map(
        make_body(mesh.shape["tp"], mesh.shape["dp"]),
        mesh=mesh,
        in_specs=placed,
        out_specs=(P(None, "dp"), P(None, None, "dp", "tp")),
        check_vma=False,
    )
```

```python
import functools
import math

import jax
import jax.numpy as jnp
from jax import lax
from jax.experimental import pallas as pl
from jax.experimental.pallas import tpu as pltpu
from jax.sharding import PartitionSpec as P


BLOCK_LEN = 256
LEN_MAX = 4096
NORM_EPS = 1e-06
F32 = jnp.float32
BF16 = jnp.bfloat16


def position_factor(lengths):
    blocks = (lengths // BLOCK_LEN).astype(F32)
    return 2.0 / (1.0 + blocks * (4.0 * BLOCK_LEN / LEN_MAX))


def exchange(value, axis, size, stride, count, k):
    pairs = []
    for i in range(size):
        digit = (i // stride) % count
        pairs.append((i, i + ((digit ^ k) - digit) * stride))
    return lax.ppermute(value, axis, pairs)


def params(mib=16):
    return pltpu.CompilerParams(vmem_limit_bytes=mib << 20)


VMEM = pl.BlockSpec(memory_space=pltpu.VMEM)
ANY = pl.BlockSpec(memory_space=pl.ANY)
HBM = pl.BlockSpec(memory_space=pltpu.HBM)


def struct(shape, dtype):
    return jax.ShapeDtypeStruct(shape, dtype)


def nt_dot(a, b):
    return lax.dot_general(a, b, (((1,), (1,)), ((), ())), preferred_element_type=F32)


def digits(inner):
    index = lax.axis_index("tp")
    return index % inner, index // inner


def call(kernel, args, outs, scratch=(), mib=4):
    return pl.pallas_call(
        kernel,
        in_specs=[VMEM] * len(args),
        out_specs=[VMEM] * len(outs),
        out_shape=outs,
        scratch_shapes=scratch,
        compiler_params=params(mib),
        cost_estimate=pl.CostEstimate(flops=1 << 22, bytes_accessed=1 << 20, transcendentals=0),
    )(*args)


def corner():
    index = lax.axis_index("tp")
    return index % 4, (index // 4) % 2, index // 8


def placed_sources(pieces, chunk):
    low, near, _ = corner()
    for k, piece in enumerate(pieces):
        if piece is not None:
            for j in range(2):
                for far in range(2):
                    at = ((2 * far + (near ^ j)) * 4 + (low ^ k)) * chunk
                    yield pl.multiple_of(at, chunk), k, piece.at[j, far]


def iota(shape, axis):
    return lax.broadcasted_iota(jnp.int32, shape, axis)


def exact_dot(a, b):
    return jnp.dot(a, b, precision=lax.Precision.HIGHEST, preferred_element_type=F32)


def prepare_kernel(
    layer, lengths_ref, step_ref, re_ref, im_ref, in_ref, out_ref, coeff_ref, m_ref, n_ref
):
    _, groups, states = re_ref.shape
    total, width = coeff_ref.shape[2], n_ref.shape[1]
    group = width // groups
    own = lengths_ref.shape[1]
    row = jnp.broadcast_to(position_factor(lengths_ref[...]), (own, own))
    factor = jnp.sum(
        jnp.where(iota((own, own), 0) == iota((own, own), 1), row, 0.0), axis=1, keepdims=True
    )
    spread = (iota((states, total), 1) % states == iota((states, total), 0)).astype(F32)
    spread_half = spread.astype(BF16)
    of_group = iota((groups, total), 1) // states == iota((groups, total), 0)
    keep = iota((width, total), 0) // group == iota((width, total), 1) // states

    def flat(value):
        return jnp.sum(
            jnp.where(of_group, exact_dot(value, spread), 0.0), axis=0, keepdims=True
        )

    log_step = exact_dot(step_ref[layer : layer + 1, :], of_group.astype(F32))
    eig_re = flat(re_ref[layer])
    eig_im = flat(im_ref[layer])
    step_size = jnp.exp(log_step) * factor
    magnitude = jnp.exp(eig_re * step_size)
    turned = eig_im * step_size
    decay_re = magnitude * jnp.cos(turned)
    decay_im = magnitude * jnp.sin(turned)
    scale = 1.0 / (eig_re * eig_re + eig_im * eig_im)
    coeff_ref[0] = decay_re
    coeff_ref[1] = decay_im
    coeff_ref[2] = ((decay_re - 1.0) * eig_re + decay_im * eig_im) * scale
    coeff_ref[3] = (decay_im * eig_re - (decay_re - 1.0) * eig_im) * scale
    for part in range(2):
        for source, target in ((in_ref, m_ref), (out_ref, n_ref)):
            value = jnp.dot(
                source[layer, part].astype(BF16), spread_half, preferred_element_type=F32
            )
            if part == 1 and target is n_ref:
                value = -value
            target[part] = jnp.where(keep, value, 0.0).astype(BF16)


def prepare(layer, own, lengths, log_step, eig_re, eig_im, in_rows, out_rows):
    _, groups, states = eig_re.shape
    total, width = groups * states, in_rows.shape[2]
    outs = [
        struct((4, own, total), F32),
        struct((2, width, total), BF16),
        struct((2, width, total), BF16),
    ]
    args = (lengths, log_step, eig_re, eig_im, in_rows, out_rows)
    return call(functools.partial(prepare_kernel, layer), args, outs)


def pack_kernel(in_hbm, glu_hbm, gate_hbm, in_out, *refs):
    packs, sem, sems = refs[:4], refs[4], refs[5]
    chunk = packs[0].shape[1] // 8
    low, _, _ = corner()
    copies = [pltpu.make_async_copy(in_hbm.at[1], in_out, sem)]
    for k in range(4):
        for w, source in enumerate((glu_hbm, gate_hbm)):
            for h in range(4):
                at = pl.multiple_of((h * 4 + (low ^ k)) * chunk, chunk)
                copies.append(
                    pltpu.make_async_copy(
                        source.at[1, :, pl.ds(at, chunk)],
                        packs[k].at[:, (w * 4 + h) * chunk : (w * 4 + h + 1) * chunk],
                        sems.at[k, w, h],
                    )
                )
    for copy in copies:
        copy.start()
    for copy in copies:
        copy.wait()


def pack(w_in, w_glu, w_gate):
    width, chunk = w_glu.shape[1], w_glu.shape[2] // 16
    args = [pltpu.with_memory_space_constraint(a, pltpu.HBM) for a in (w_in, w_glu, w_gate)]
    outs = [pltpu.VMEM(w_in.shape[1:], BF16)] + [pltpu.VMEM((width, 8 * chunk), BF16)] * 4
    return pl.pallas_call(
        pack_kernel,
        in_specs=[HBM] * 3,
        out_specs=[VMEM] * 5,
        out_shape=outs,
        scratch_shapes=[pltpu.SemaphoreType.DMA, pltpu.SemaphoreType.DMA((4, 2, 4))],
        compiler_params=params(4),
        cost_estimate=pl.CostEstimate(flops=8 << 20, bytes_accessed=3 << 20, transcendentals=0),
        name="pack",
    )(*args)


def project_kernel(count, *refs):
    tokens_hbm, gain_hbm, weight_hbm = refs[:3]
    sources, (keep, send), targets = refs[3 : 3 + count], refs[3 + count : 5 + count], refs[5 + count : -4]
    tokens, gain, weight, sems = refs[-4:]
    pairs = [(tokens_hbm, tokens), (gain_hbm, gain), (weight_hbm.at[0], weight)]
    pairs += [(a.at[0] if len(a.shape) > len(b.shape) else a, b) for a, b in zip(sources, targets)]
    copies = [pltpu.make_async_copy(a, b, sems.at[i]) for i, (a, b) in enumerate(pairs)]
    for copy in copies:
        copy.start()
    own, width = keep.shape[0], weight.shape[1]
    chunk = tokens.shape[1] // 16
    copies[0].wait()
    copies[1].wait()
    current = tokens[...].astype(F32)
    squares = jnp.sum(current * current, axis=1, keepdims=True)
    scaled = (current * gain[0:1, :]).astype(BF16)
    copies[2].wait()
    term = jnp.dot(scaled, weight[...], preferred_element_type=F32)
    low, near, _ = corner()
    me = lax.axis_index("dp")
    for out, flip in ((keep, me), (send, 1 - me)):
        upper = flip == 1
        out[:, :width] = jnp.where(upper, term[own:], term[:own])
        out[:, width : width + 128] = jnp.broadcast_to(
            jnp.where(upper, squares[own:], squares[:own]), (own, 128)
        )
        start = pl.multiple_of(flip * own, own)
        for far in range(2):
            at = pl.multiple_of(((2 * far + near) * 4 + low) * chunk, chunk)
            base = width + 128 + far * chunk
            out[:, base : base + chunk] = tokens[pl.ds(start, own), pl.ds(at, chunk)].astype(F32)
    for copy in copies[3:]:
        copy.wait()


def project(dims, tokens, gain, weight, others, stacks):
    _, _, _, _, own, feats = dims
    width = weight.shape[2]
    shape = (own, width + 128 + 2 * feats // 16)
    args = [pltpu.with_memory_space_constraint(a, pltpu.HBM) for a in (tokens, gain, weight, *others, *stacks)]
    made = pl.pallas_call(
        functools.partial(project_kernel, len(others) + len(stacks)),
        in_specs=[HBM] * len(args),
        out_specs=[VMEM] * (2 + len(others) + len(stacks)),
        out_shape=[struct(shape, F32)] * 2 + [pltpu.VMEM(a.shape, a.dtype) for a in others]
        + [pltpu.VMEM(a.shape[1:], a.dtype) for a in stacks],
        scratch_shapes=[
            pltpu.VMEM(tokens.shape, BF16),
            pltpu.VMEM(gain.shape, F32),
            pltpu.VMEM(weight.shape[1:], BF16),
            pltpu.SemaphoreType.DMA((len(args),)),
        ],
        compiler_params=params(4),
        cost_estimate=pl.CostEstimate(flops=32 << 20, bytes_accessed=1 << 20, transcendentals=0),
        name="project",
    )(*args)
    return made[0], made[1], made[2 : 2 + len(others)], made[2 + len(others) :]


def piece_kernel(k, dp, layer, piece, *refs):
    gains, weights, (partial_out, squares_out) = refs[:dp], refs[dp : 2 * dp], refs[2 * dp :]
    own, chunk = piece.shape[2], piece.shape[3] // dp
    low, near, _ = corner()
    squares = jnp.zeros((own, 1), F32)
    partial_value = jnp.zeros(partial_out.shape, F32)
    for j in range(2):
        for far in range(2):
            at = ((2 * far + (near ^ j)) * 4 + (low ^ k)) * chunk
            at = pl.multiple_of(at, chunk)
            for p in range(dp):
                current = piece[j, far, :, p * chunk : (p + 1) * chunk].astype(F32)
                squares = squares + jnp.sum(current * current, axis=1, keepdims=True)
                gain = gains[p][layer : layer + 1, pl.ds(at, chunk)]
                scaled = (current * gain).astype(BF16)
                partial_value = partial_value + jnp.dot(
                    scaled, weights[p][pl.ds(at, chunk), :], preferred_element_type=F32
                )
    partial_out[...] = partial_value
    squares_out[...] = jnp.broadcast_to(squares, squares_out.shape)


def project_piece(k, layer, piece, gains, weights):
    own = piece.shape[2]
    dp = len(gains)
    width = weights[0].shape[1]
    return call(
        functools.partial(piece_kernel, k, dp, layer),
        (piece, *gains, *weights),
        [struct((own, width), F32), struct((own, 128), F32)],
    )


def recur_kernel(layer, dp, model, *refs):
    coeff_ref, m_ref, n_ref, skip_ref, state_ref = refs[:5]
    width = skip_ref.shape[1]
    if layer == 0:
        pieces, (readout_ref, new_ref, before_ref) = refs[5:7], refs[7:]
        chunk = before_ref.shape[2] // dp
        partial_value = pieces[0][:, :width] + pieces[1][:, :width]
        squares = (pieces[0][:, width : width + 128] + pieces[1][:, width : width + 128])[:, :1]
        for far in range(2):
            for p in range(dp):
                base = width + 128 + far * chunk
                before_ref[far, :, p * chunk : (p + 1) * chunk] = pieces[p][
                    :, base : base + chunk
                ].astype(BF16)
    else:
        terms, (readout_ref, new_ref) = refs[5:13], refs[13:]
        partial_value = terms[0][...] + terms[2][...] + terms[4][...] + terms[6][...]
        squares = terms[1][...] + terms[3][...] + terms[5][...] + terms[7][...]
        squares = squares[:, :1]
    driven = (partial_value * lax.rsqrt(squares / model + NORM_EPS)).astype(BF16)
    drive_re = jnp.dot(driven, m_ref[0], preferred_element_type=F32)
    drive_im = jnp.dot(driven, m_ref[1], preferred_element_type=F32)
    decay_re, decay_im = coeff_ref[0], coeff_ref[1]
    weight_re, weight_im = coeff_ref[2], coeff_ref[3]
    old_re, old_im = state_ref[layer, 0], state_ref[layer, 1]
    new_re = decay_re * old_re - decay_im * old_im + weight_re * drive_re - weight_im * drive_im
    new_im = decay_re * old_im + decay_im * old_re + weight_re * drive_im + weight_im * drive_re
    new_ref[0] = new_re
    new_ref[1] = new_im
    value = nt_dot(new_re.astype(BF16), n_ref[0])
    value = value + nt_dot(new_im.astype(BF16), n_ref[1])
    value = value + skip_ref[layer : layer + 1, :] * driven.astype(F32)
    readout_ref[...] = jax.nn.gelu(value).astype(BF16)


def recur(layer, dims, consts, terms):
    dp, _, _, model, own, feats = dims
    skip, state = consts[3:]
    outs = [struct((own, skip.shape[1]), BF16), pltpu.VMEM(state.shape[1:], F32)]
    if layer == 0:
        outs.append(struct((2, own, dp * feats // 16), BF16))
    return call(functools.partial(recur_kernel, layer, dp, model), (*consts, *terms), outs, mib=8)


def store_kernel(first, second, out, sems):
    copies = [
        pltpu.make_async_copy(ref, out.at[layer], sems.at[layer])
        for layer, ref in enumerate((first, second))
    ]
    for copy in copies:
        copy.start()
    for copy in copies:
        copy.wait()


def store(states):
    return pl.pallas_call(
        store_kernel,
        in_specs=[VMEM] * 2,
        out_specs=ANY,
        out_shape=struct((2,) + states[0].shape, F32),
        scratch_shapes=[pltpu.SemaphoreType.DMA((2,))],
        compiler_params=params(4),
        cost_estimate=pl.CostEstimate(flops=1 << 20, bytes_accessed=1 << 19, transcendentals=0),
        name="store",
    )(*states)


def half_kernel(chunk, readout_ref, *refs):
    weights, spread = refs[:-1], refs[-1]
    for w, ref in enumerate(weights):
        value = jnp.dot(readout_ref[...], ref[...], preferred_element_type=F32)
        for j in range(16):
            spread[w, j] = value[:, j * chunk : (j + 1) * chunk]


def product_kernel(chunk, readout_ref, mine, *refs):
    weights, outs, theirs = refs[:2], refs[2:6], refs[6]
    low, _, _ = corner()
    half_kernel(chunk, readout_ref, *weights, theirs)
    for k in range(4):
        for h in range(4):
            for w in range(4):
                source = (mine, theirs)[w % 2]
                outs[k][h, :, w * chunk : (w + 1) * chunk] = source[
                    w // 2, h * 4 + (low ^ k)
                ].astype(outs[k].dtype)


def products(dims, readout, weights):
    _, _, _, _, own, feats = dims
    chunk = feats // 16
    shape = (4, own, len(weights) * chunk)
    half = (2, 16, own, chunk)
    (mine,) = call(
        functools.partial(half_kernel, chunk),
        (readout, weights[0], weights[2]),
        [struct(half, F32)],
    )
    return call(
        functools.partial(product_kernel, chunk),
        (readout, mine, weights[1], weights[3]),
        [struct(shape, F32)] + [struct(shape, BF16)] * 3,
        [pltpu.VMEM(half, F32)],
        8,
    )


def gathered_kernel(chunk, *refs):
    readouts, weights, (keep, send, spread) = refs[:4], refs[4:8], refs[8:]
    _, near, _ = corner()
    value = None
    for k in range(4):
        term = jnp.dot(readouts[k][...], weights[k][...], preferred_element_type=F32)
        value = term if value is None else value + term
    for j in range(8):
        spread[j] = value[:, j * chunk : (j + 1) * chunk]
    for far in range(2):
        for w in range(2):
            lanes = slice(w * chunk, (w + 1) * chunk)
            at = w * 4 + 2 * far + near
            keep[far, :, lanes] = spread[at]
            send[far, :, lanes] = spread[w * 4 + 2 * far + (near ^ 1)].astype(BF16)


def gathered_products(chunk, readouts, weights):
    rows = readouts[0].shape[0]
    return call(
        functools.partial(gathered_kernel, chunk),
        (*readouts, *weights),
        [struct((2, rows, 2 * chunk), F32), struct((2, rows, 2 * chunk), BF16)],
        [pltpu.VMEM((8, rows, chunk), F32)],
        8,
    )


def fold_low_kernel(own_ref, a_ref, b_ref, c_ref, keep, send):
    _, near, _ = corner()
    for far in range(2):
        for out, turn in ((keep, 0), (send, 1)):
            at = 2 * far + (near ^ turn)
            total = own_ref[at] + a_ref[at].astype(F32) + b_ref[at].astype(F32)
            out[far] = (total + c_ref[at].astype(F32)).astype(out.dtype)


def fold_near_kernel(own_ref, arrived_ref, send):
    send[...] = (own_ref[...] + arrived_ref[...].astype(F32)).astype(BF16)


def updated(own_ref, arrived_ref, before_ref):
    total = own_ref[...].astype(F32) + arrived_ref[...].astype(F32)
    half = total.shape[2] // 2
    linear, gate = total[:, :, :half], total[:, :, half:]
    return (before_ref[...].astype(F32) + linear * jax.nn.sigmoid(gate)).astype(BF16)


def update_kernel(own_ref, arrived_ref, before_ref, out):
    out[...] = updated(own_ref, arrived_ref, before_ref)


def merge_kernel(own_ref, arrived_ref, out):
    rows = own_ref.shape[1]
    me = lax.axis_index("dp")
    half = out.shape[2]
    out[:, pl.ds(pl.multiple_of(me * rows, rows), rows), :] = own_ref[:, :, :half]
    out[:, pl.ds(pl.multiple_of((1 - me) * rows, rows), rows), :] = arrived_ref[...]


def settle_kernel(which, chunk, *refs):
    pieces, out, sem = refs[: len(which)], refs[-2], refs[-1]
    slots = [None] * 4
    for k, piece in zip(which, pieces):
        slots[k] = piece
    copies = []
    for at, k, source in placed_sources(slots, chunk):
        copies.append(
            pltpu.make_async_copy(source, out.at[:, pl.ds(at, chunk)], sem.at[len(copies)])
        )
        copies[-1].start()
    for copy in copies:
        copy.wait()


def settle(which, pieces, feats, so_far=None):
    rows, chunk = pieces[0].shape[2:]
    args = [pieces[k] for k in which]
    specs = [VMEM] * len(args)
    alias = {}
    if so_far is not None:
        alias = {len(args): 0}
        args.append(so_far)
        specs.append(ANY)
    return pl.pallas_call(
        functools.partial(settle_kernel, which, chunk),
        in_specs=specs,
        out_specs=ANY,
        out_shape=struct((rows, feats), BF16),
        scratch_shapes=[pltpu.SemaphoreType.DMA((4 * len(which),))],
        input_output_aliases=alias,
        compiler_params=params(4),
        cost_estimate=pl.CostEstimate(flops=1 << 20, bytes_accessed=1 << 18, transcendentals=0),
        name="settle",
    )(*args)


def plain_prepare(lengths, log_step, eig_re, eig_im, in_mat, output_matrices):
    factor = position_factor(lengths)
    step_size = jnp.exp(log_step)[:, None, :, None] * factor[None, :, None, None]
    eig_re, eig_im = eig_re[:, None], eig_im[:, None]
    magnitude = jnp.exp(eig_re * step_size)
    turned = eig_im * step_size
    decay_re = magnitude * jnp.cos(turned)
    decay_im = magnitude * jnp.sin(turned)
    modulus = eig_re * eig_re + eig_im * eig_im
    weight_re = ((decay_re - 1.0) * eig_re + decay_im * eig_im) / modulus
    weight_im = (decay_im * eig_re - (decay_re - 1.0) * eig_im) / modulus
    return jnp.stack([decay_re, decay_im, weight_re, weight_im], axis=1), in_mat, output_matrices


def plain_order(pieces, inner, outer):
    low, high = digits(inner)
    rows = []
    for h in range(outer):
        for l in range(inner):
            row = jnp.stack(pieces)[low ^ l, high ^ h]
            rows.append(row)
    return jnp.stack(rows)


def plain_recur(layer, dims, pieces, gains, weights, coeff, m, n, skip, state, so_far):
    dp, inner, outer, model, own, feats = dims
    groups, states = coeff.shape[3:]
    if layer > 0:
        rows = plain_order(pieces, inner, outer)
        rows = rows.reshape(inner * outer, own, dp, feats // (inner * outer))
        pieces = [rows[:, :, p].transpose(1, 0, 2).reshape(own, feats) for p in range(dp)]
    else:
        start = lax.axis_index("dp") * own
        pieces = [lax.dynamic_slice_in_dim(p, start, own, axis=0) for p in pieces]
    squares, partial_value = 0.0, 0.0
    for p in range(dp):
        current = pieces[p].astype(F32)
        squares = squares + jnp.sum(current * current, axis=1, keepdims=True)
        scaled = (current * gains[p][layer]).astype(BF16)
        partial_value = partial_value + jnp.dot(
            scaled, weights[p][layer], preferred_element_type=F32
        )
    driven = (partial_value * lax.rsqrt(squares / model + NORM_EPS)).astype(BF16).astype(F32)
    driven = driven.reshape(own, groups, -1)
    exact = lax.Precision.HIGHEST
    drive_re = jnp.einsum("bgc,gpc->bgp", driven, m[layer, 0], precision=exact)
    drive_im = jnp.einsum("bgc,gpc->bgp", driven, m[layer, 1], precision=exact)
    decay_re, decay_im, weight_re, weight_im = [coeff[layer, c] for c in range(4)]
    old_re, old_im = [state[layer, c].reshape(own, groups, states) for c in range(2)]
    new_re = decay_re * old_re - decay_im * old_im + weight_re * drive_re - weight_im * drive_im
    new_im = decay_re * old_im + decay_im * old_re + weight_re * drive_im + weight_im * drive_re
    value = jnp.einsum("bgp,gcp->bgc", new_re, n[layer, 0], precision=exact)
    value = value - jnp.einsum("bgp,gcp->bgc", new_im, n[layer, 1], precision=exact)
    value = value + skip[layer].reshape(groups, -1) * driven
    readout = jax.nn.gelu(value).reshape(own, -1).astype(BF16)
    new = jnp.stack([new_re, new_im]).reshape(1, 2, own, groups * states)
    if layer > 0:
        return readout, jnp.concatenate([so_far, new])
    chunk = feats // (inner * outer)
    start = lax.axis_index("tp") * chunk
    cuts = [lax.dynamic_slice_in_dim(p, start, chunk, axis=1) for p in pieces]
    return readout, new, jnp.concatenate(cuts, axis=1)


def plain_products(layer, dims, readout, weights):
    _, inner, outer, _, own, _ = dims
    terms = []
    for w in weights:
        term = jnp.dot(readout, w[layer], preferred_element_type=F32)
        terms.append(term.reshape(own, outer, inner, -1))
    terms = jnp.concatenate(terms, axis=3).transpose(2, 1, 0, 3)
    low, _ = digits(inner)
    outs = [terms[low ^ k] for k in range(inner)]
    return [outs[0]] + [o.astype(BF16) for o in outs[1:]]


def plain_fold(value, arrived):
    for a in arrived:
        value = value + a.astype(F32)
    _, high = digits(len(arrived) + 1)
    outs = [value[high ^ k] for k in range(value.shape[0])]
    return [outs[0]] + [o.astype(BF16) for o in outs[1:]]


def plain_update(block, arrived, before):
    for a in arrived:
        block = block + a.astype(F32)
    half = block.shape[1] // 2
    gated = block[:, :half] * jax.nn.sigmoid(block[:, half:])
    return (before.astype(F32) + gated).astype(BF16)


def plain_settle(pieces, feats):
    rows = plain_order(pieces, len(pieces), pieces[0].shape[0])
    return rows.transpose(1, 0, 2).reshape(rows.shape[1], feats)


def plain_layers(dims, layers, pieces, slabs_of, pointwise):
    dp, inner, outer, _, own, feats = dims
    gain_slabs, in_slabs, out_slabs = slabs_of
    lengths, log_step, eig_re, eig_im, in_mat, output_matrices, skip, state = pointwise
    tp = inner * outer
    chunk = feats // tp

    def over_low(value, k):
        return exchange(value, "tp", tp, 1, inner, k)

    def over_high(value, k):
        return exchange(value, "tp", tp, inner, outer, k)

    coeff, m, n = plain_prepare(lengths, log_step, eig_re, eig_im, in_mat, output_matrices)
    new_state = None
    for layer in range(layers):
        made = plain_recur(
            layer, dims, pieces, gain_slabs, in_slabs, coeff, m, n, skip, state, new_state
        )
        readout, new_state = made[:2]
        if layer == 0:
            before = made[2]
        sends = plain_products(layer, dims, readout, out_slabs)
        arrived = [over_low(sends[k], k) for k in range(1, inner)]
        sends = plain_fold(sends[0], arrived)
        arrived = [over_high(sends[k], k) for k in range(1, outer)]
        shard = plain_update(sends[0], arrived, before)
        before = shard
        if layer + 1 == layers:
            cuts = [shard[:, k * chunk : (k + 1) * chunk] for k in range(dp)]
            here = [cuts[0]] + [exchange(cuts[k], "dp", dp, 1, dp, k) for k in range(1, dp)]
            order = lax.axis_index("dp") ^ jnp.arange(dp)
            shard = jnp.stack(here)[order].reshape(own * dp, chunk)
        column = jnp.stack([shard] + [over_high(shard, k) for k in range(1, outer)])
        pieces = [column] + [over_low(column, k) for k in range(1, inner)]
    return plain_settle(pieces, feats), new_state


def kernel_layers(dims, tokens, norm_gain, w_in, w_glu, w_gate, pointwise):
    dp, _, _, _, own, feats = dims
    lengths, log_step, eig_re, eig_im, in_mat, output_matrices, skip, state = pointwise
    layers = w_in.shape[0]
    chunk = feats // 16
    wide = 2 * dp * chunk

    def core_swap(value):
        return exchange(value, "dp", 2, 1, 2, 1)

    def over_low(value, k):
        return exchange(value, "tp", 16, 1, 4, k)

    def over_near(value):
        return exchange(value, "tp", 16, 4, 2, 1)

    def over_far(value):
        return exchange(value, "tp", 16, 8, 2, 1)

    width = skip.shape[1]
    others = (
        lengths[None, :],
        log_step,
        eig_re,
        eig_im,
        jnp.swapaxes(in_mat, 3, 4).reshape(layers, 2, width, -1),
        output_matrices.reshape(layers, 2, width, -1),
        skip,
    )
    keep, send, others, outward = project(
        dims, tokens, norm_gain, w_in, others, (w_glu, w_gate)
    )
    pieces = [keep, core_swap(send)]
    outward = [outward[0], core_swap(outward[0]), outward[1], core_swap(outward[1])]
    consts = (*prepare(0, own, *others[:6]), *others[6:], state)

    readout, new_first, before = recur(0, dims, consts, pieces)
    parts = products(dims, readout, outward)
    arrived = [over_low(parts[k], k) for k in range(1, 4)]
    stacks = lax.optimization_barrier((w_in, w_glu, w_gate, norm_gain, parts[0]))
    inward, *packs = pack(*stacks[:3])
    gain = stacks[3]
    *others, _ = lax.optimization_barrier((*others, parts[0]))
    later_consts = (*prepare(1, own, *others[:6]), *others[6:], state)
    slabs = [norm_gain, core_swap(gain), inward, core_swap(inward)]
    keep, send = call(
        fold_low_kernel,
        (parts[0], *arrived),
        [struct((2, own, wide), F32), struct((2, own, wide), BF16)],
    )
    arrived = over_near(send)
    *packs, _ = lax.optimization_barrier((*packs, send))
    weights = [packs[0]] + [over_low(packs[k], k) for k in range(1, 4)]
    (send,) = call(fold_near_kernel, (keep, arrived), [struct((2, own, wide), BF16)])
    terms = (send, over_far(send), before)
    (shard,) = call(update_kernel, terms, [struct((2, own, dp * chunk), BF16)])
    column = jnp.stack([shard, over_near(shard)])
    pieces = [column] + [over_low(column, k) for k in range(1, 4)]
    away, _ = lax.optimization_barrier((shard[:, :, chunk:], column))
    away = core_swap(away)
    (before,) = call(merge_kernel, (shard, away), [struct((2, own * dp, chunk), BF16)])

    terms = []
    for k in (0, 3, 2, 1):
        terms += project_piece(k, 1, pieces[k], slabs[:2], slabs[2:])
    readout, new_second = recur(1, dims, later_consts, terms)
    readout = readout[None]
    (rows,) = call(
        merge_kernel, (readout, core_swap(readout)), [struct((1, own * dp, width), BF16)]
    )
    rows = rows[0]
    readouts = [rows] + [over_low(rows, k) for k in range(1, 4)]
    keep, send = gathered_products(chunk, readouts, weights)
    arrived = over_near(send)
    (send,) = call(fold_near_kernel, (keep, arrived), [struct((2, own * dp, 2 * chunk), BF16)])
    new_state = store([new_first, new_second])
    terms = (send, over_far(send), before)
    (shard,) = call(update_kernel, terms, [struct((2, own * dp, chunk), BF16)])
    column = jnp.stack([shard, over_near(shard)])
    pieces = [column] + [over_low(column, k) for k in range(1, 4)]
    mixed = settle((0, 3), pieces, feats)
    return settle((1, 2), pieces, feats, mixed), new_state


def make_body(tp, dp):
    inner = 1 << (int(math.log2(tp)) // 2)
    outer = tp // inner

    def body(
        tokens,
        lengths,
        norm_gain,
        w_in,
        log_step,
        eig_re,
        eig_im,
        in_mat,
        output_matrices,
        skip,
        w_glu,
        w_gate,
        state,
    ):
        layers = w_in.shape[0]
        seqs, feats = tokens.shape
        own = seqs // dp
        chunk = feats // tp
        dims = (dp, inner, outer, feats * dp, own, feats)
        pointwise = (lengths, log_step, eig_re, eig_im, in_mat, output_matrices, skip, state)
        regular = tp == 16 and dp == 2 and layers == 2 and chunk % 128 == 0 and own % 16 == 0
        if regular and skip.shape[1] % 128 == 0:
            return kernel_layers(dims, tokens, norm_gain, w_in, w_glu, w_gate, pointwise)

        def slabs(value):
            return [value] + [exchange(value, "dp", dp, 1, dp, k) for k in range(1, dp)]

        slabs_of = (slabs(norm_gain), slabs(w_in), slabs(w_glu) + slabs(w_gate))
        return plain_layers(dims, layers, slabs(tokens), slabs_of, pointwise)

    return body


def solution(mesh):
    placed = (
        P(None, "dp"),
        P("dp"),
        P(None, "dp"),
        P(None, "dp", "tp"),
        P(None, "tp"),
        P(None, "tp", None),
        P(None, "tp", None),
        P(None, None, "tp", None, None),
        P(None, None, "tp", None, None),
        P(None, "tp"),
        P(None, "tp", "dp"),
        P(None, "tp", "dp"),
        P(None, None, "dp", "tp"),
    )
    return jax.shard_map(
        make_body(mesh.shape["tp"], mesh.shape["dp"]),
        mesh=mesh,
        in_specs=placed,
        out_specs=(P(None, "dp"), P(None, None, "dp", "tp")),
        check_vma=False,
    )
```
